512 devices in a mesh: ep: 32 (over z, core), tp: 16 (over y, x).
Axes of the slice: x: 4, y: 4, z: 16, core: 2. Of those that a mesh axis runs over, the one named last changes fastest.
Arguments:
- query_maps: bfloat16 [8192, 4096], P('ep', 'tp'), may hold values from -40 to 40
- key_maps: bfloat16 [8192, 4096], P('ep', 'tp'), may hold values from -40 to 40
- value_rows: bfloat16 [8192, 4096], P('ep', 'tp'), may hold values from -6 to 6
- head_lambda: float32 [16], P('tp'), may hold values from 0.3 to 0.8
- head_gain: float32 [256], replicated, may hold values from 0.1 to 1.9
- out_weight: bfloat16 [4096, 2048], P('tp'), may hold values from -0.125 to 0.125
- expert_rows: bfloat16 [4096, 2048], P('ep'), may hold values from -6 to 6
- expert_gain: float32 [2048], replicated, may hold values from 0.1 to 1.9
- routes: int32 [4096, 2], P('ep'), may hold values from 0 to 31, all different within a row; in each aligned block of 128 rows (0 to 127, 128 to 255, ...) at most 12 rows name the same one
- route_weights: float32 [4096, 2], P('ep'), may hold values from 0.2 to 1
- gate_weight: bfloat16 [32, 2048, 4096], P('ep', None, 'tp'), may hold values from -0.125 to 0.125
- up_weight: bfloat16 [32, 2048, 4096], P('ep', None, 'tp'), may hold values from -0.125 to 0.125
- down_weight: bfloat16 [32, 4096, 2048], P('ep', 'tp'), may hold values from -0.125 to 0.125
Outputs:
- mixed: bfloat16 [8192, 2048], P('ep', 'tp')
- expert_out: bfloat16 [4096, 2048], P('ep', 'tp')
The draws below stay inside these ranges and needn't reach their ends.
Inputs may be any that keep to these rules, and one draw needn't show every extreme that they name: `routes`: within the rows of one device (aligned blocks of 128 rows) no expert is named more than 12 times, and the 2 experts of a row differ.
All inputs are finite; a program needn't handle non-finite values.
Results may differ from the reference program's by a relative error of at most 0.018.
Values may be sent and summed in bfloat16 or wider, within the bound.
No kernel may reach another device: no remote copies, remote signals or barrier semaphores. Data moves between devices by JAX's collectives and lax.ppermute only.
A program may use at most 128 MiB of HBM per device.

```python
import math
import jax
import jax.numpy as jnp
import numpy as np
from jax import lax

D = 2048
HEADS = 16
HEAD = 128
VHEAD = 256
FF = 4096
TOPK = 2
MOE_DEV = 128
TOKENS = 8192
MOE_TOK = 4096
EXPERTS = 32
CAP = 12
N_EP = 32
N_TP = 16


def draw_query_maps(key, part):
    base = jnp.clip(1.3 * jax.random.normal(jax.random.fold_in(key, 1), (TOKENS, HEADS * 2 * HEAD), jnp.float32), -7.8, 7.8)
    return base.astype(jnp.bfloat16)


def draw_key_maps(key, part):
    base = jnp.clip(1.3 * jax.random.normal(jax.random.fold_in(key, 2), (TOKENS, HEADS * 2 * HEAD), jnp.float32), -7.8, 7.8)
    base = base.reshape(TOKENS, HEADS, 2, HEAD)
    return base.reshape(TOKENS, HEADS * 2 * HEAD).astype(jnp.bfloat16)


def spiked(result, own_key, source, target, shards_of, factor):
    owner, partner = [(jnp.arange(result.shape[axis_at]) // (result.shape[axis_at] // shards_of)).reshape([-1 if axis == axis_at else 1 for axis in range(result.ndim)]) for axis_at in (source, target)]
    chosen = jax.random.permutation(own_key, shards_of)[partner]
    strong = (owner == chosen) | (owner == (partner + shards_of // 2) % shards_of)
    return jnp.where(strong, factor * result, result)


def level_of(stream_key, dims, cuts, low, top_value):
    loudness = 1.0
    for axis_at, blocks in cuts:
        steps = jax.random.uniform(jax.random.fold_in(jax.random.fold_in(stream_key, 6), axis_at), (blocks,), jnp.float32, low / len(cuts), top_value / len(cuts))
        loudness = loudness * jnp.repeat(jnp.exp(steps), dims[axis_at] // blocks).reshape((-1,) + (1,) * (len(dims) - 1 - axis_at))
    return loudness


def routed_block(stream_key, own, number, rows, amount, top, most, skew):
    order = jax.random.permutation(stream_key, amount)
    heavy_load, ordinary = load_shares(amount, rows * top, most, skew, True), load_shares(amount, rows * top, most, skew, False)
    places = jnp.arange(amount)

    def named(sizes, turn):
        used = int((sizes > 0).sum())
        fixed = max(1, used // 4)
        passed = fixed + (places - fixed + turn * (used - fixed)) % max(1, amount - fixed)
        return jnp.zeros((amount,), jnp.int32).at[order[jnp.where(places < fixed, places, passed)]].set(jnp.asarray(sizes, jnp.int32))

    sizes = jnp.where(number % 4 == 0, named(heavy_load, number // 4), named(ordinary, number - number // 4 - 1))
    mixed = jax.random.permutation(jax.random.fold_in(own, 3), amount)
    source_of, receiver = mixed[0:amount // 2 * 2:2], mixed[1:amount // 2 * 2:2]
    room = jnp.minimum(sizes[source_of] - 1, most - sizes[receiver]) // 2
    room = jnp.where((source_of == order[0]) | (receiver == order[0]) | (sizes[receiver] == 0), 0, jnp.maximum(room, 0))
    passed = jax.random.randint(jax.random.fold_in(own, 4), (amount // 2,), 0, 1 << 20) % (room + 1)
    sizes = sizes.at[source_of].add(-passed).at[receiver].add(passed)
    labels = jnp.searchsorted(jnp.cumsum(sizes), jnp.arange(rows * top), side="right").astype(jnp.int32)
    table = labels.reshape(top, rows).T
    table = table[jax.random.permutation(jax.random.fold_in(own, 1), rows)]
    turn = jax.random.randint(jax.random.fold_in(own, 2), (rows, 1), 0, top)
    return jnp.take_along_axis(table, (jnp.arange(top)[None, :] + turn) % top, axis=1)


def load_shares(number_of, total, bound, lean, full):
    portions = [(1 << 20) // math.isqrt(standing ** lean) + 1 for standing in range(1, number_of + 1)]
    largest = bound if full else min(bound, max(-(-total // number_of), total * portions[0] // sum(portions)))
    least = 1 if total - largest >= number_of - 1 else 0
    holding, surplus = [largest] + [least] * (number_of - 1), total - largest - least * (number_of - 1)
    while surplus > 0:
        free = [i for i in range(1, number_of) if holding[i] < largest] or [i for i in range(1, number_of) if holding[i] < bound]
        mass, budget = sum([portions[i] for i in free]), surplus
        for i in free:
            extra = min(bound - holding[i], max(1, budget * portions[i] // mass), surplus)
            holding[i] = holding[i] + extra
            surplus = surplus - extra
    return np.array(holding)


def centred(rng, extent, spread, bound, cuts=(), kind=jnp.bfloat16):
    array = spread * jax.random.normal(rng, extent, jnp.float32)
    if cuts:
        array = array * level_of(rng, extent, cuts, -0.22, 0.18)
    return jnp.clip(array, -bound, bound).astype(kind)


def heavy_noise(rng, extent, scale, most, split, heavy, kind=jnp.bfloat16):
    array = scale * jax.random.normal(rng, extent, jnp.float32)
    if split:
        array = array * level_of(rng, extent, split, -0.22, 0.18)
    return jnp.clip(spiked(array, jax.random.fold_in(rng, 3), *heavy), -most, most).astype(kind)


def setup_inputs(seed: int = 0) -> dict:
    key_list = jax.random.split(jax.random.key(seed), 14)
    query_maps = draw_query_maps(jax.random.fold_in(key_list[13], 71), 0)
    key_maps = draw_key_maps(jax.random.fold_in(key_list[13], 71), 0)
    value_rows = centred(key_list[2], (TOKENS, HEADS * VHEAD), 1.0, 6.0, ((0, 32), (1, 16)))
    head_lambda = jnp.clip(0.3 + 0.5 * jax.random.uniform(key_list[3], (HEADS,), jnp.float32) ** level_of(key_list[3], (HEADS,), ((0, 16),), -0.2, 0.2), 0.3, 0.8)
    head_gain = jnp.clip(1.0 + 0.18 * jax.random.normal(key_list[4], (VHEAD,), jnp.float32), 0.1, 1.9)
    out_weight = heavy_noise(key_list[5], (HEADS * VHEAD, D), (HEADS * VHEAD) ** -0.5, 0.125, ((0, 16),), (0, 1, 16, 2.0))
    expert_rows = centred(key_list[6], (MOE_TOK, D), 1.0, 6.0, ((0, 32),))
    expert_gain = jnp.clip(1.0 + 0.18 * jax.random.normal(key_list[7], (D,), jnp.float32), 0.1, 1.9)
    routes_keys = jax.random.split(jax.random.fold_in(key_list[8], 1), MOE_TOK // MOE_DEV)
    routes_turns = jax.random.permutation(jax.random.fold_in(key_list[8], 3), MOE_TOK // MOE_DEV)
    routes = jax.vmap(lambda own, number: routed_block(jax.random.fold_in(key_list[8], 2), own, number, MOE_DEV, EXPERTS, TOPK, CAP, 2))(routes_keys, routes_turns).reshape((MOE_TOK, TOPK))
    route_weights = jnp.clip(0.2 + 0.8 * jax.random.uniform(key_list[9], (MOE_TOK, TOPK), jnp.float32) ** level_of(key_list[9], (MOE_TOK, TOPK), ((0, 32),), -0.2, 0.2), 0.2, 1.0)
    gate_weight = centred(key_list[10], (EXPERTS, D, FF), D ** -0.5, 0.125, ((0, 32), (2, 16)))
    up_weight = centred(key_list[11], (EXPERTS, D, FF), D ** -0.5, 0.125, ((0, 32), (2, 16)))
    down_weight = heavy_noise(key_list[12], (EXPERTS, FF, D), FF ** -0.5, 0.125, ((0, 32), (1, 16)), (1, 2, 16, 2.0))
    return dict(query_maps=query_maps, key_maps=key_maps, value_rows=value_rows, head_lambda=head_lambda, head_gain=head_gain, out_weight=out_weight, expert_rows=expert_rows, expert_gain=expert_gain, routes=routes, route_weights=route_weights, gate_weight=gate_weight, up_weight=up_weight, down_weight=down_weight)


norm_eps = 1e-06
rope_base = 10000.0

def rope_turn(inputs, positions):
    half_dim = inputs.shape[-1] // 2
    inverse = rope_base ** (-2.0 * jnp.arange(half_dim, dtype=jnp.float32) / inputs.shape[-1])
    angles = positions.astype(jnp.float32)[:, None] * inverse[None, :]
    cos_table = jnp.cos(angles)[:, None, None, :]
    sin_table = jnp.sin(angles)[:, None, None, :]
    first_half = inputs[..., :half_dim]
    second_half = inputs[..., half_dim:]
    return jnp.concatenate([first_half * cos_table - second_half * sin_table, second_half * cos_table + first_half * sin_table], axis=-1)

def mixer_half(query_maps, key_maps, value_rows, head_lambda, head_gain, out_weight):
    positions = jnp.arange(TOKENS, dtype=jnp.int32)
    rotated_q = rope_turn(query_maps.astype(jnp.float32).reshape(TOKENS, HEADS, 2, HEAD), positions).astype(jnp.bfloat16)
    rotated_k = rope_turn(key_maps.astype(jnp.float32).reshape(TOKENS, HEADS, 2, HEAD), positions).astype(jnp.bfloat16)
    values_all = value_rows.reshape(TOKENS, HEADS, VHEAD)
    block_size = math.gcd(512, TOKENS)
    score_scale = HEAD ** (-0.5)

    def one_head(head_index):
        head_q = rotated_q[:, head_index].astype(jnp.float32)
        head_k = rotated_k[:, head_index].astype(jnp.float32)
        head_v = values_all[:, head_index].astype(jnp.float32)
        key_pos = jnp.arange(TOKENS, dtype=jnp.int32)

        def one_block(block_index):
            first_row = (block_index * block_size).astype(jnp.int32)
            block_q = lax.dynamic_slice_in_dim(head_q, first_row, block_size, 0)
            query_pos = first_row + jnp.arange(block_size, dtype=jnp.int32)
            scores = jnp.einsum('qmd,kmd->mqk', block_q, head_k) * score_scale
            causal = (key_pos[None, :] <= query_pos[:, None])[None]
            masked = jnp.where(causal, scores, -jnp.inf)
            peak = lax.optimization_barrier(jnp.max(masked, axis=-1, keepdims=True))
            expd = jnp.where(causal, jnp.exp(masked - peak), 0.0)
            probs = expd / lax.optimization_barrier(jnp.sum(expd, axis=-1, keepdims=True))
            rounded = lax.optimization_barrier(probs.astype(jnp.bfloat16))
            map_out = jnp.einsum('mqk,ke->mqe', rounded.astype(jnp.float32), head_v)
            difference = map_out[0] - head_lambda[head_index] * map_out[1]
            normed = difference * lax.rsqrt(lax.optimization_barrier(jnp.mean(difference * difference, axis=-1, keepdims=True)) + norm_eps) * head_gain
            return normed.astype(jnp.bfloat16)
        blocks = lax.map(one_block, jnp.arange(TOKENS // block_size, dtype=jnp.int32))
        return blocks.reshape(TOKENS, VHEAD)
    per_head = lax.map(one_head, jnp.arange(HEADS, dtype=jnp.int32))
    group_size = HEADS // N_TP
    grouped = per_head.reshape(N_TP, group_size, TOKENS, VHEAD)
    weight_groups = out_weight.reshape(N_TP, group_size, VHEAD, D)

    def add_group(running, pieces):
        group_heads, group_weight = pieces
        partial_value = jnp.einsum('hte,hed->td', group_heads.astype(jnp.float32), group_weight.astype(jnp.float32))
        rounded = lax.optimization_barrier(partial_value.astype(jnp.bfloat16))
        return (running + rounded.astype(jnp.float32), None)
    summed, _ = lax.scan(add_group, jnp.zeros((TOKENS, D), jnp.float32), (grouped, weight_groups))
    return summed.astype(jnp.bfloat16)

def expert_half(expert_rows, expert_gain, routes, route_weights, gate_weight, up_weight, down_weight):
    inputs = expert_rows.astype(jnp.float32)
    normed = (inputs * lax.rsqrt(lax.optimization_barrier(jnp.mean(inputs * inputs, axis=-1, keepdims=True)) + norm_eps) * expert_gain).astype(jnp.bfloat16)
    expert_ids = routes.reshape(N_EP, MOE_DEV * TOPK)
    one_hot = (expert_ids[..., None] == jnp.arange(EXPERTS, dtype=jnp.int32)).astype(jnp.int32)
    slot_index = lax.optimization_barrier(jnp.sum((jnp.cumsum(one_hot, axis=1) - one_hot) * one_hot, axis=-1)).astype(jnp.int32)
    source_block = jnp.zeros_like(expert_ids) + jnp.arange(N_EP, dtype=jnp.int32)[:, None]
    repeated = jnp.repeat(normed.reshape(N_EP, MOE_DEV, D), TOPK, axis=1)
    buffer = jnp.zeros((EXPERTS, N_EP, CAP, D), normed.dtype).at[expert_ids, source_block, slot_index].set(repeated)
    group_width = FF // N_TP

    def run_one(pieces):
        slots, gate_one, up_one, down_one = pieces
        flat_rows = slots.reshape(N_EP * CAP, D)
        gate_values = jnp.dot(flat_rows, gate_one, preferred_element_type=jnp.float32)
        up_values = jnp.dot(flat_rows, up_one, preferred_element_type=jnp.float32)
        hidden = (jax.nn.silu(gate_values) * up_values).astype(jnp.bfloat16)
        hidden_groups = jnp.transpose(hidden.reshape(N_EP * CAP, N_TP, group_width), (1, 0, 2))
        down_groups = down_one.reshape(N_TP, group_width, D)

        def add_group(running, pieces_inner):
            hidden_part, down_part = pieces_inner
            partial_value = jnp.dot(hidden_part, down_part, preferred_element_type=jnp.float32)
            rounded = lax.optimization_barrier(partial_value.astype(jnp.bfloat16))
            return (running + rounded.astype(jnp.float32), None)
        summed, _ = lax.scan(add_group, jnp.zeros((N_EP * CAP, D), jnp.float32), (hidden_groups, down_groups))
        return summed.astype(jnp.bfloat16).reshape(N_EP, CAP, D)
    results = lax.map(run_one, (buffer, gate_weight, up_weight, down_weight))
    picked = results[expert_ids, source_block, slot_index].reshape(MOE_TOK, TOPK, D)
    combined = lax.optimization_barrier(jnp.sum(route_weights[..., None] * picked.astype(jnp.float32), axis=1))
    return combined.astype(jnp.bfloat16)

def reference(query_maps, key_maps, value_rows, head_lambda, head_gain, out_weight, expert_rows, expert_gain, routes, route_weights, gate_weight, up_weight, down_weight):
    mixed = mixer_half(query_maps, key_maps, value_rows, head_lambda, head_gain, out_weight)
    expert_out = expert_half(expert_rows, expert_gain, routes, route_weights, gate_weight, up_weight, down_weight)
    return (mixed, expert_out)
```

```python
import functools

import jax
import jax.numpy as jnp
from jax import lax
from jax.experimental import pallas as pl
from jax.experimental.pallas import tpu as pltpu
from jax.sharding import PartitionSpec as P

norm_eps = 1e-06
rope_base = 10000.0
low = -1e30
log2e = 1.4426950408889634


def vmem(count):
    return [pl.BlockSpec(memory_space=pltpu.VMEM) for _ in range(count)]


def smem(count):
    return [pl.BlockSpec(memory_space=pltpu.SMEM) for _ in range(count)]


def dot_f32(a, b, dims):
    return lax.dot_general(a, b, (dims, ((), ())), preferred_element_type=jnp.float32)


def turn_kernel(q_ref, k_ref, v_ref, cos_ref, sin_ref, q_out, kv_out):
    cos_table = cos_ref[...]
    sin_table = sin_ref[...]

    def turned(x):
        x = x.astype(jnp.float32)
        return (x * cos_table + pltpu.roll(x, 64, 1) * sin_table).astype(jnp.bfloat16)

    for m in range(2):
        at = slice(128 * m, 128 * (m + 1))
        q_out[:, at] = turned(q_ref[:, at])
        kv_out[:, at] = turned(k_ref[:, at])
    kv_out[:, 256:] = v_ref[...]


def turn(q, k, v, offset):
    rows = q.shape[0]
    lane = jnp.arange(128, dtype=jnp.int32)
    inverse = rope_base ** (-2.0 * (lane % 64).astype(jnp.float32) / 128)
    positions = (offset + jnp.arange(rows, dtype=jnp.int32)).astype(jnp.float32)
    angles = positions[:, None] * inverse[None, :]
    cos_table = jnp.cos(angles)
    sin_table = jnp.sin(angles) * jnp.where(lane < 64, -1.0, 1.0)[None, :]
    return pl.pallas_call(
        turn_kernel,
        out_shape=(
            jax.ShapeDtypeStruct((rows, 256), jnp.bfloat16),
            jax.ShapeDtypeStruct((rows, 512), jnp.bfloat16),
        ),
        in_specs=vmem(5),
        out_specs=tuple(vmem(2)),
        name="turn",
    )(q, k, v, cos_table, sin_table)


def reaches(ep, source):
    way, distance = source
    if way == "below":
        return ep // 2 >= distance
    return ep // 2 + distance >= 16


def flash_kernel(sources, ep_ref, own_q, other_q, *refs):
    count = len(sources)
    blocks, outs, scores_ref = refs[:count], refs[count : count + 2], refs[-1]
    factor = (128.0**-0.5) * log2e
    ep = ep_ref[0]
    for half, (q_ref, out) in enumerate(zip((own_q, other_q), outs)):
        for m in range(2):
            q = q_ref[:, 128 * m : 128 * (m + 1)]
            running = jnp.full((256, 128), low, jnp.float32)
            for j, (block, source) in enumerate(zip(blocks, sources)):
                s = dot_f32(q, block[:, 128 * m : 128 * (m + 1)], ((1,), (1,)))
                if source[0] == "own" and half == 0:
                    row = lax.broadcasted_iota(jnp.int32, (256, 256), 0)
                    col = lax.broadcasted_iota(jnp.int32, (256, 256), 1)
                    s = jnp.where(col <= row, s, low)
                scores_ref[:, 256 * j : 256 * (j + 1)] = s
                top = jnp.maximum(s[:, :128], s[:, 128:])
                if source[0] == "own":
                    top = top if half == 0 else jnp.where(ep % 2 == 0, top, low)
                else:
                    top = jnp.where(reaches(ep, source), top, low)
                running = jnp.maximum(running, top)
            peak = jnp.max(running, axis=1, keepdims=True) * factor
            total = jnp.zeros((256, 128), jnp.float32)
            acc = jnp.zeros((256, 256), jnp.float32)
            for j, (block, source) in enumerate(zip(blocks, sources)):
                if source[0] == "own":
                    base = peak if half == 0 else jnp.where(ep % 2 == 0, peak, -low)
                else:
                    base = jnp.where(reaches(ep, source), peak, -low)
                p = jnp.exp2(scores_ref[:, 256 * j : 256 * (j + 1)] * factor - base)
                total = total + (p[:, :128] + p[:, 128:])
                acc = acc + dot_f32(p.astype(jnp.bfloat16), block[:, 256:], ((1,), (0,)))
            mass = jnp.sum(total, axis=1, keepdims=True)
            out[m, :, :256] = acc
            lane = lax.broadcasted_iota(jnp.int32, (256, 128), 1)
            out[m, :, 256:] = jnp.where(lane < 64, peak, mass)


def flash(ep, own_q, other_q, named):
    sources = tuple(source for source, _ in named)
    count = len(named)
    state_shape = jax.ShapeDtypeStruct((2, 256, 384), jnp.float32)
    return pl.pallas_call(
        functools.partial(flash_kernel, sources),
        out_shape=(state_shape, state_shape),
        in_specs=smem(1) + vmem(2 + count),
        out_specs=tuple(vmem(2)),
        scratch_shapes=[pltpu.VMEM((256, 256 * count), jnp.float32)],
        cost_estimate=pl.CostEstimate(
            flops=2 * 512 * 256 * count * 2 * 512,
            transcendentals=512 * 256 * count * 2,
            bytes_accessed=256 * 1024 * count,
        ),
        name="flash",
    )(ep, own_q, other_q, *(block for _, block in named))


def project_kernel(lam_ref, *refs):
    states, (gain_ref, weight_ref, out_ref) = refs[:-3], refs[-3:]
    maps = []
    for m in range(2):
        peaks = [state[m, :, 256:257] for state in states]
        peak = functools.reduce(jnp.maximum, peaks)
        mass, acc = 0.0, 0.0
        for state, own_peak in zip(states, peaks):
            scale = jnp.exp2(own_peak - peak)
            mass = mass + scale * state[m, :, 320:321]
            acc = acc + scale * state[m, :, :256]
        maps.append(acc / mass)
    difference = maps[0] - lam_ref[0] * maps[1]
    mean = jnp.mean(difference * difference, axis=1, keepdims=True)
    head = (difference * lax.rsqrt(mean + norm_eps) * gain_ref[...]).astype(jnp.bfloat16)
    for j in range(8):
        part = dot_f32(head, weight_ref[:, 256 * j : 256 * (j + 1)], ((1,), (0,)))
        part = part.astype(jnp.bfloat16)
        out_ref[2 * j] = part[:, :128]
        out_ref[2 * j + 1] = part[:, 128:]


def project(lam, states, gain, weight):
    return pl.pallas_call(
        project_kernel,
        out_shape=jax.ShapeDtypeStruct((16, 256, 128), jnp.bfloat16),
        in_specs=smem(1) + vmem(len(states) + 2),
        out_specs=vmem(1)[0],
        name="project",
    )(lam, *states, gain.reshape(1, 256), weight)


def slots_of(routes_ref):
    expert = lax.broadcasted_iota(jnp.int32, (32, 128), 0)
    first = routes_ref[0:1, :] == expert
    second = routes_ref[1:2, :] == expert
    named = jnp.where(first | second, 1.0, 0.0).astype(jnp.bfloat16)
    before = lax.broadcasted_iota(jnp.int32, (128, 128), 0)
    after = lax.broadcasted_iota(jnp.int32, (128, 128), 1)
    earlier = jnp.where(before < after, 1.0, 0.0).astype(jnp.bfloat16)
    slot = dot_f32(named, earlier, ((1,), (0,))).astype(jnp.int32)
    return first, second, slot


def chosen(named, slot):
    where = jnp.where(named, slot, -1)[:, None, :]
    index = lax.broadcasted_iota(jnp.int32, (32, 16, 128), 1)
    return jnp.where(where == index, 1.0, 0.0).reshape(512, 128).astype(jnp.bfloat16)


def pack_kernel(tp_ref, rows_ref, gain_ref, routes_ref, out_ref):
    x = rows_ref[...].astype(jnp.float32)
    inverse = lax.rsqrt(jnp.mean(x * x, axis=1, keepdims=True) + norm_eps)
    start = pl.multiple_of(tp_ref[0] * 128, 128)
    mine = rows_ref[:, pl.ds(start, 128)].astype(jnp.float32)
    normed = (mine * inverse * gain_ref[:, pl.ds(start, 128)]).astype(jnp.bfloat16)
    first, second, slot = slots_of(routes_ref)
    pick = chosen(first | second, slot)
    packed = dot_f32(pick, normed, ((1,), (0,)))
    out_ref[...] = packed.astype(jnp.bfloat16).reshape(32, 16, 128)


def pack(tp, rows, gain, routes_t):
    return pl.pallas_call(
        pack_kernel,
        out_shape=jax.ShapeDtypeStruct((32, 16, 128), jnp.bfloat16),
        in_specs=smem(1) + vmem(3),
        out_specs=vmem(1)[0],
        name="pack",
    )(tp, rows, gain.reshape(1, -1), routes_t)


def dense_slots(shape, slot_dim):
    slot = lax.broadcasted_iota(jnp.int32, shape, slot_dim)
    row = lax.broadcasted_iota(jnp.int32, shape, 1 - slot_dim)
    place = jnp.where((slot & 15) < 12, (slot >> 4) * 12 + (slot & 15), -1)
    return jnp.where(place == row, 1.0, 0.0).astype(jnp.bfloat16)


def squeeze_kernel(arrived_ref, out_ref):
    slots = arrived_ref[...].reshape(512, 128)
    rows = dot_f32(dense_slots((384, 512), 1), slots, ((1,), (0,))).astype(jnp.bfloat16)
    for j in range(16):
        out_ref[j] = rows


def squeeze(arrived):
    return pl.pallas_call(
        squeeze_kernel,
        out_shape=jax.ShapeDtypeStruct((16, 384, 128), jnp.bfloat16),
        in_specs=vmem(1),
        out_specs=vmem(1)[0],
        name="squeeze",
    )(arrived)


def ffn_kernel(rows_ref, gate_ref, up_ref, down_ref, out_ref):
    gate = jnp.zeros((384, 256), jnp.float32)
    up = jnp.zeros((384, 256), jnp.float32)
    for j in range(8):
        x = jnp.concatenate([rows_ref[2 * j], rows_ref[2 * j + 1]], axis=1)
        at = slice(256 * j, 256 * (j + 1))
        gate = gate + dot_f32(x, gate_ref[at, :], ((1,), (0,)))
        up = up + dot_f32(x, up_ref[at, :], ((1,), (0,)))
    hidden = (gate / (1.0 + jnp.exp(-gate)) * up).astype(jnp.bfloat16)
    for j in range(8):
        part = dot_f32(hidden, down_ref[:, 256 * j : 256 * (j + 1)], ((1,), (0,)))
        part = part.astype(jnp.bfloat16)
        out_ref[2 * j] = part[:, :128]
        out_ref[2 * j + 1] = part[:, 128:]


def ffn(rows, gate, up, down):
    return pl.pallas_call(
        ffn_kernel,
        out_shape=jax.ShapeDtypeStruct((16, 384, 128), jnp.bfloat16),
        in_specs=vmem(4),
        out_specs=vmem(1)[0],
        cost_estimate=pl.CostEstimate(
            flops=2 * 384 * 2048 * 768, transcendentals=384 * 256, bytes_accessed=6 * 2**20
        ),
        name="ffn",
    )(rows, gate, up, down)


def total_kernel(parts_ref, out_ref):
    total = parts_ref[0].astype(jnp.float32)
    for j in range(1, 16):
        total = total + parts_ref[j].astype(jnp.float32)
    rows = total.astype(jnp.bfloat16)
    slots = dot_f32(dense_slots((512, 384), 0), rows, ((1,), (0,)))
    out_ref[...] = slots.astype(jnp.bfloat16).reshape(32, 16, 128)


def total_of(parts):
    return pl.pallas_call(
        total_kernel,
        out_shape=jax.ShapeDtypeStruct((32, 16, 128), jnp.bfloat16),
        in_specs=vmem(1),
        out_specs=vmem(1)[0],
        name="total",
    )(parts)


def combine_kernel(returned_ref, routes_ref, weights_ref, out_ref):
    slots = returned_ref[...].reshape(512, 128)
    first, second, slot = slots_of(routes_ref)
    one = dot_f32(chosen(first, slot), slots, ((0,), (0,)))
    two = dot_f32(chosen(second, slot), slots, ((0,), (0,)))
    out = weights_ref[:, 0:1] * one + weights_ref[:, 1:2] * two
    out_ref[...] = out.astype(jnp.bfloat16)


def combine(returned, routes_t, weights):
    return pl.pallas_call(
        combine_kernel,
        out_shape=jax.ShapeDtypeStruct((128, 128), jnp.bfloat16),
        in_specs=vmem(3),
        out_specs=vmem(1)[0],
        name="combine",
    )(returned, routes_t, weights)


def exchange(blocks, axis):
    return lax.all_to_all(blocks, axis, split_axis=0, concat_axis=0, tiled=True)


def on_device(
    query_maps,
    key_maps,
    value_rows,
    head_lambda,
    head_gain,
    out_weight,
    expert_rows,
    expert_gain,
    routes,
    route_weights,
    gate_weight,
    up_weight,
    down_weight,
):
    ep = lax.axis_index("ep")
    tp = lax.axis_index("tp")
    depth = lax.axis_size("ep") // 2
    swap = [(i, i ^ 1) for i in range(2 * depth)]
    tied = lax.optimization_barrier

    routes_t = routes.T
    packed = pack(tp.reshape(1), expert_rows, expert_gain, routes_t)
    own_q, own_kv = turn(query_maps, key_maps, value_rows, ep * query_maps.shape[0])
    packed, own_q, own_kv = tied((packed, own_q, own_kv))
    arrived = exchange(packed, "ep")
    forward, backward = [own_kv], [own_kv]

    def step(r):
        up = [(2 * (s - 1) + c, 2 * s + c) for s in range(r, depth) for c in range(2)]
        forward.append(lax.ppermute(forward[-1], "ep", up))
        if r < depth // 2:
            ends = [(b - r) % depth for b in range(depth // 2 - 1)]
            down = [(2 * ((s + 1) % depth) + c, 2 * s + c) for s in ends for c in range(2)]
            backward.append(lax.ppermute(backward[-1], "ep", down))

    step(1)
    step(2)
    other_q = lax.ppermute(own_q, "ep", swap)
    arrived, forward[-1], backward[-1] = tied((arrived, forward[-1], backward[-1]))
    gathered = exchange(squeeze(arrived), "tp")
    step(3)
    step(4)
    step(5)
    gathered, forward[-1], backward[-1] = tied((gathered, forward[-1], backward[-1]))
    parts = ffn(gathered, gate_weight[0], up_weight[0], down_weight[0])
    arrived_parts = exchange(parts, "tp")
    step(6)
    forward[-1], backward[-1], parts = tied((forward[-1], backward[-1], parts))
    step(7)
    step(8)

    index = ep.reshape(1)

    def block_group(rounds):
        return [
            ((way, r), blocks[r])
            for r in rounds
            for way, blocks in (("below", forward), ("above", backward))
            if r < len(blocks)
        ]

    first, first_other = flash(
        index, own_q, other_q, [(("own", 0), own_kv)] + block_group(range(1, 6))
    )
    theirs_first = lax.ppermute(first_other, "ep", swap)
    summed = total_of(arrived_parts)
    last_f, summed = tied((forward[-1], summed))
    forward[-1] = last_f
    returned = exchange(summed, "ep")
    second, second_other = flash(index, own_q, other_q, block_group(range(6, 9)))
    theirs_second = lax.ppermute(second_other, "ep", swap)
    states = (first, theirs_first, second, theirs_second)
    partial_value = project(head_lambda, states, head_gain, out_weight)
    mixed_parts = exchange(partial_value, "tp")
    mixed = mixed_parts.astype(jnp.float32).sum(axis=0).astype(jnp.bfloat16)
    expert_out = combine(returned, routes_t, route_weights)
    return (mixed, expert_out)


def solution(mesh):
    placed = (
        P("ep", "tp"),
        P("ep", "tp"),
        P("ep", "tp"),
        P("tp"),
        P(),
        P("tp", None),
        P("ep", None),
        P(),
        P("ep", None),
        P("ep", None),
        P("ep", None, "tp"),
        P("ep", None, "tp"),
        P("ep", "tp", None),
    )
    return jax.shard_map(
        on_device,
        mesh=mesh,
        in_specs=placed,
        out_specs=(P("ep", "tp"), P("ep", "tp")),
        check_vma=False,
    )
```

```python
import functools

import jax
import jax.numpy as jnp
from jax import lax
from jax.experimental import pallas as pl
from jax.experimental.pallas import tpu as pltpu
from jax.sharding import PartitionSpec as P


norm_eps = 1e-06
rope_base = 10000.0
low = -1e30
log2e = 1.4426950408889634


def vmem(count):
    return [pl.BlockSpec(memory_space=pltpu.VMEM) for _ in range(count)]


def near(x):
    return pltpu.with_memory_space_constraint(x, pltpu.VMEM)


def far(x):
    return pltpu.with_memory_space_constraint(x, pltpu.HBM)


def hbm(count):
    return [pl.BlockSpec(memory_space=pltpu.HBM) for _ in range(count)]


def start_copies(sources, targets, semaphores):
    copies = [
        pltpu.make_async_copy(a, b, semaphores.at[i])
        for i, (a, b) in enumerate(zip(sources, targets))
    ]
    for copy in copies:
        copy.start()
    return copies


def smem(count):
    return [pl.BlockSpec(memory_space=pltpu.SMEM) for _ in range(count)]


def dot_f32(a, b, dims):
    return lax.dot_general(a, b, (dims, ((), ())), preferred_element_type=jnp.float32)


def turn_kernel(q_hbm, k_hbm, v_hbm, cos_ref, sin_ref, q_out, kv_out, q_ref, k_ref, semaphores):
    copies = start_copies(
        (q_hbm, k_hbm, v_hbm), (q_ref, k_ref, kv_out.at[:, pl.ds(256, 256)]), semaphores
    )
    cos_table = cos_ref[...]
    sin_table = sin_ref[...]

    def turned(x):
        x = x.astype(jnp.float32)
        return (x * cos_table + pltpu.roll(x, 64, 1) * sin_table).astype(jnp.bfloat16)

    for ref, out, copy in ((q_ref, q_out, copies[0]), (k_ref, kv_out, copies[1])):
        copy.wait()
        for m in range(2):
            at = slice(128 * m, 128 * (m + 1))
            out[:, at] = turned(ref[:, at])
    copies[2].wait()


def turn(q, k, v, offset):
    rows = q.shape[0]
    lane = jnp.arange(128, dtype=jnp.int32)
    inverse = rope_base ** (-2.0 * (lane % 64).astype(jnp.float32) / 128)
    positions = (offset + jnp.arange(rows, dtype=jnp.int32)).astype(jnp.float32)
    angles = positions[:, None] * inverse[None, :]
    cos_table = jnp.cos(angles)
    sin_table = jnp.sin(angles) * jnp.where(lane < 64, -1.0, 1.0)[None, :]
    return pl.pallas_call(
        turn_kernel,
        out_shape=(
            pltpu.VMEM((rows, 256), jnp.bfloat16),
            pltpu.VMEM((rows, 512), jnp.bfloat16),
        ),
        compiler_params=pltpu.CompilerParams(vmem_limit_bytes=24 * 2**20),
        in_specs=hbm(3) + vmem(2),
        out_specs=tuple(vmem(2)),
        scratch_shapes=[
            pltpu.VMEM((rows, 256), jnp.bfloat16),
            pltpu.VMEM((rows, 256), jnp.bfloat16),
            pltpu.SemaphoreType.DMA((3,)),
        ],
        name="turn",
    )(far(q), far(k), far(v), near(cos_table), near(sin_table))


chunk = 1024


def attend_kernel(ep_ref, lam_ref, *refs):
    sources, refs = refs[:4], refs[4:]
    kv_hbm = sources[3]
    out_ref, q_ref, weight_ref, gain_ref, kv_buf, top_ref, mass_ref, acc_ref = refs[:8]
    semaphores, kv_semaphores = refs[8:]
    ep = ep_ref[0]
    full = ep * 256 // chunk
    factor = (128.0**-0.5) * log2e
    copies = start_copies((sources[0],), (q_ref,), semaphores)

    def chunk_copy(j):
        at = pl.ds(pl.multiple_of(j * chunk, chunk), chunk)
        return pltpu.make_async_copy(kv_hbm.at[at, :], kv_buf.at[j], kv_semaphores.at[j])

    lax.fori_loop(0, full + 1, lambda j, c: (chunk_copy(j).start(), c)[1], 0)
    late = start_copies(
        sources[1:3], (weight_ref, gain_ref), semaphores.at[pl.ds(1, 2)]
    )
    top_ref[...] = jnp.full(top_ref.shape, low, jnp.float32)
    mass_ref[...] = jnp.zeros(mass_ref.shape, jnp.float32)
    acc_ref[...] = jnp.zeros(acc_ref.shape, jnp.float32)
    copies[0].wait()

    def fold(j, masked):
        for m in range(2):
            q = q_ref[:, 128 * m : 128 * (m + 1)]
            s = dot_f32(q, kv_buf[j, :, 128 * m : 128 * (m + 1)], ((1,), (1,)))
            if masked:
                row = ep * 256 + lax.broadcasted_iota(jnp.int32, (256, chunk), 0)
                col = j * chunk + lax.broadcasted_iota(jnp.int32, (256, chunk), 1)
                s = jnp.where(col <= row, s, low)
            pieces = [s[:, 128 * i : 128 * (i + 1)] for i in range(chunk // 128)]
            peak = jnp.max(functools.reduce(jnp.maximum, pieces), axis=1, keepdims=True)
            before = top_ref[m, :, 0:1]
            peak = jnp.maximum(peak * factor, before)
            rescale = jnp.exp2(before - peak)
            top_ref[m] = jnp.broadcast_to(peak, (256, 128))
            p = jnp.exp2(s * factor - peak)
            pieces = [p[:, 128 * i : 128 * (i + 1)] for i in range(chunk // 128)]
            mass_ref[m] = mass_ref[m] * rescale + functools.reduce(jnp.add, pieces)
            gained = dot_f32(p.astype(jnp.bfloat16), kv_buf[j, :, 256:], ((1,), (0,)))
            acc_ref[m] = acc_ref[m] * rescale + gained

    def step(j, c):
        chunk_copy(j).wait()
        fold(j, False)
        return c

    lax.fori_loop(0, full, step, 0)
    chunk_copy(full).wait()
    fold(full, True)
    maps = [acc_ref[m] / jnp.sum(mass_ref[m], axis=1, keepdims=True) for m in range(2)]
    difference = maps[0] - lam_ref[0] * maps[1]
    mean = jnp.mean(difference * difference, axis=1, keepdims=True)
    for copy in late:
        copy.wait()
    head = (difference * lax.rsqrt(mean + norm_eps) * gain_ref[...]).astype(jnp.bfloat16)
    for j in range(8):
        part = dot_f32(head, weight_ref[:, 256 * j : 256 * (j + 1)], ((1,), (0,)))
        part = part.astype(jnp.bfloat16)
        out_ref[2 * j] = part[:, :128]
        out_ref[2 * j + 1] = part[:, 128:]


def attend(ep, lam, q, kv, gain, weight):
    return pl.pallas_call(
        attend_kernel,
        out_shape=pltpu.VMEM((16, 256, 128), jnp.bfloat16),
        compiler_params=pltpu.CompilerParams(vmem_limit_bytes=40 * 2**20),
        in_specs=smem(2) + hbm(4),
        out_specs=vmem(1)[0],
        scratch_shapes=[
            pltpu.VMEM((256, 256), jnp.bfloat16),
            pltpu.VMEM(weight.shape, jnp.bfloat16),
            pltpu.VMEM((1, 256), jnp.float32),
            pltpu.VMEM((kv.shape[0] // chunk, chunk, 512), jnp.bfloat16),
            pltpu.VMEM((2, 256, 128), jnp.float32),
            pltpu.VMEM((2, 256, 128), jnp.float32),
            pltpu.VMEM((2, 256, 256), jnp.float32),
            pltpu.SemaphoreType.DMA((3,)),
            pltpu.SemaphoreType.DMA((kv.shape[0] // chunk,)),
        ],
        cost_estimate=pl.CostEstimate(
            flops=2 * 256 * kv.shape[0] * 2 * 512,
            transcendentals=256 * kv.shape[0] * 2,
            bytes_accessed=kv.shape[0] * 1024,
        ),
        name="attend",
    )(ep, lam, far(q), far(weight), far(gain.reshape(1, 256)), far(kv))


def slots_of(routes_ref):
    expert = lax.broadcasted_iota(jnp.int32, (32, 128), 0)
    first = routes_ref[0:1, :] == expert
    second = routes_ref[1:2, :] == expert
    named = jnp.where(first | second, 1.0, 0.0).astype(jnp.bfloat16)
    before = lax.broadcasted_iota(jnp.int32, (128, 128), 0)
    after = lax.broadcasted_iota(jnp.int32, (128, 128), 1)
    earlier = jnp.where(before < after, 1.0, 0.0).astype(jnp.bfloat16)
    slot = dot_f32(named, earlier, ((1,), (0,))).astype(jnp.int32)
    return first, second, slot


def chosen(named, slot):
    where = jnp.where(named, slot, -1)[:, None, :]
    index = lax.broadcasted_iota(jnp.int32, (32, 16, 128), 1)
    return jnp.where(where == index, 1.0, 0.0).reshape(512, 128).astype(jnp.bfloat16)


def pack_kernel(tp_ref, *refs):
    sources, (out_ref, rows_ref, gain_ref, routes_ref, semaphores) = refs[:3], refs[3:]
    copies = start_copies(sources, (rows_ref, gain_ref, routes_ref), semaphores)
    copies[2].wait()
    first, second, slot = slots_of(routes_ref)
    pick = chosen(first | second, slot)
    copies[0].wait()
    copies[1].wait()
    x = rows_ref[...].astype(jnp.float32)
    inverse = lax.rsqrt(jnp.mean(x * x, axis=1, keepdims=True) + norm_eps)
    start = pl.multiple_of(tp_ref[0] * 128, 128)
    mine = rows_ref[:, pl.ds(start, 128)].astype(jnp.float32)
    normed = (mine * inverse * gain_ref[:, pl.ds(start, 128)]).astype(jnp.bfloat16)
    packed = dot_f32(pick, normed, ((1,), (0,)))
    out_ref[...] = packed.astype(jnp.bfloat16).reshape(32, 16, 128)


def pack(tp, rows, gain, routes_t):
    return pl.pallas_call(
        pack_kernel,
        out_shape=pltpu.VMEM((32, 16, 128), jnp.bfloat16),
        compiler_params=pltpu.CompilerParams(vmem_limit_bytes=24 * 2**20),
        in_specs=smem(1) + hbm(3),
        out_specs=vmem(1)[0],
        scratch_shapes=[
            pltpu.VMEM(rows.shape, jnp.bfloat16),
            pltpu.VMEM((1, rows.shape[1]), jnp.float32),
            pltpu.VMEM(routes_t.shape, jnp.int32),
            pltpu.SemaphoreType.DMA((3,)),
        ],
        name="pack",
    )(tp, far(rows), far(gain.reshape(1, -1)), far(routes_t))


def dense_slots(shape, slot_dim):
    slot = lax.broadcasted_iota(jnp.int32, shape, slot_dim)
    row = lax.broadcasted_iota(jnp.int32, shape, 1 - slot_dim)
    place = jnp.where((slot & 15) < 12, (slot >> 4) * 12 + (slot & 15), -1)
    return jnp.where(place == row, 1.0, 0.0).astype(jnp.bfloat16)


def squeeze_kernel(arrived_ref, out_ref):
    slots = arrived_ref[...].reshape(512, 128)
    rows = dot_f32(dense_slots((384, 512), 1), slots, ((1,), (0,))).astype(jnp.bfloat16)
    for j in range(16):
        out_ref[j] = rows


def squeeze(arrived):
    return pl.pallas_call(
        squeeze_kernel,
        out_shape=pltpu.VMEM((16, 384, 128), jnp.bfloat16),
        compiler_params=pltpu.CompilerParams(vmem_limit_bytes=24 * 2**20),
        in_specs=vmem(1),
        out_specs=vmem(1)[0],
        name="squeeze",
    )(near(arrived))


def ffn_kernel(rows_ref, *refs):
    sources, (out_ref, gate_ref, up_ref, down_ref, semaphores) = refs[:3], refs[3:]
    copies = start_copies(sources, (gate_ref, up_ref, down_ref), semaphores)
    gate = jnp.zeros((384, 256), jnp.float32)
    up = jnp.zeros((384, 256), jnp.float32)
    copies[0].wait()
    for j in range(8):
        x = jnp.concatenate([rows_ref[2 * j], rows_ref[2 * j + 1]], axis=1)
        gate = gate + dot_f32(x, gate_ref[256 * j : 256 * (j + 1), :], ((1,), (0,)))
    copies[1].wait()
    for j in range(8):
        x = jnp.concatenate([rows_ref[2 * j], rows_ref[2 * j + 1]], axis=1)
        up = up + dot_f32(x, up_ref[256 * j : 256 * (j + 1), :], ((1,), (0,)))
    copies[2].wait()
    hidden = (gate / (1.0 + jnp.exp(-gate)) * up).astype(jnp.bfloat16)
    for j in range(8):
        part = dot_f32(hidden, down_ref[:, 256 * j : 256 * (j + 1)], ((1,), (0,)))
        part = part.astype(jnp.bfloat16)
        out_ref[2 * j] = part[:, :128]
        out_ref[2 * j + 1] = part[:, 128:]


def ffn(rows, gate, up, down):
    return pl.pallas_call(
        ffn_kernel,
        out_shape=pltpu.VMEM((16, 384, 128), jnp.bfloat16),
        compiler_params=pltpu.CompilerParams(vmem_limit_bytes=24 * 2**20),
        in_specs=vmem(1) + hbm(3),
        out_specs=vmem(1)[0],
        scratch_shapes=[
            pltpu.VMEM(gate.shape, jnp.bfloat16),
            pltpu.VMEM(up.shape, jnp.bfloat16),
            pltpu.VMEM(down.shape, jnp.bfloat16),
            pltpu.SemaphoreType.DMA((3,)),
        ],
        cost_estimate=pl.CostEstimate(
            flops=2 * 384 * 2048 * 768, transcendentals=384 * 256, bytes_accessed=6 * 2**20
        ),
        name="ffn",
    )(near(rows), far(gate), far(up), far(down))


def total_kernel(parts_ref, out_ref):
    total = parts_ref[0].astype(jnp.float32)
    for j in range(1, 16):
        total = total + parts_ref[j].astype(jnp.float32)
    rows = total.astype(jnp.bfloat16)
    slots = dot_f32(dense_slots((512, 384), 0), rows, ((1,), (0,)))
    out_ref[...] = slots.astype(jnp.bfloat16).reshape(32, 16, 128)


def total_of(parts):
    return pl.pallas_call(
        total_kernel,
        out_shape=pltpu.VMEM((32, 16, 128), jnp.bfloat16),
        compiler_params=pltpu.CompilerParams(vmem_limit_bytes=24 * 2**20),
        in_specs=vmem(1),
        out_specs=vmem(1)[0],
        name="total",
    )(near(parts))


def combine_kernel(returned_ref, routes_ref, weights_ref, out_ref):
    slots = returned_ref[...].reshape(512, 128)
    first, second, slot = slots_of(routes_ref)
    one = dot_f32(chosen(first, slot), slots, ((0,), (0,)))
    two = dot_f32(chosen(second, slot), slots, ((0,), (0,)))
    out = weights_ref[:, 0:1] * one + weights_ref[:, 1:2] * two
    out_ref[...] = out.astype(jnp.bfloat16)


def combine(returned, routes_t, weights):
    return pl.pallas_call(
        combine_kernel,
        out_shape=jax.ShapeDtypeStruct((128, 128), jnp.bfloat16),
        compiler_params=pltpu.CompilerParams(vmem_limit_bytes=24 * 2**20),
        in_specs=vmem(3),
        out_specs=vmem(1)[0],
        name="combine",
    )(near(returned), routes_t, weights)


def exchange(blocks, axis):
    return lax.all_to_all(blocks, axis, split_axis=0, concat_axis=0, tiled=True)


def on_device(
    query_maps,
    key_maps,
    value_rows,
    head_lambda,
    head_gain,
    out_weight,
    expert_rows,
    expert_gain,
    routes,
    route_weights,
    gate_weight,
    up_weight,
    down_weight,
):
    return step_of(
        query_maps,
        key_maps,
        value_rows,
        head_lambda,
        head_gain,
        out_weight,
        expert_rows,
        expert_gain,
        routes,
        route_weights,
        gate_weight[0],
        up_weight[0],
        down_weight[0],
    )


def step_of(
    query_maps,
    key_maps,
    value_rows,
    head_lambda,
    head_gain,
    out_weight,
    expert_rows,
    expert_gain,
    routes,
    route_weights,
    gate_weight,
    up_weight,
    down_weight,
):
    ep = lax.axis_index("ep")
    tp = lax.axis_index("tp")
    routes_t = routes.T
    packed = pack(tp.reshape(1), expert_rows, expert_gain, routes_t)
    arrived = exchange(packed, "ep")
    own_q, own_kv = turn(query_maps, key_maps, value_rows, ep * query_maps.shape[0])
    kv = lax.all_gather(own_kv, "ep", axis=0, tiled=True)
    gathered = exchange(squeeze(arrived), "tp")
    parts = ffn(gathered, gate_weight, up_weight, down_weight)
    summed = total_of(exchange(parts, "tp"))
    returned = exchange(summed, "ep")

    partial_value = attend(ep.reshape(1), head_lambda, own_q, kv, head_gain, out_weight)
    mixed_parts = exchange(partial_value, "tp")
    mixed = mixed_parts.astype(jnp.float32).sum(axis=0).astype(jnp.bfloat16)
    expert_out = combine(returned, routes_t, route_weights)
    return (mixed, expert_out)


def solution(mesh):
    placed = (
        P("ep", "tp"),
        P("ep", "tp"),
        P("ep", "tp"),
        P("tp"),
        P(),
        P("tp", None),
        P("ep", None),
        P(),
        P("ep", None),
        P("ep", None),
        P("ep", None, "tp"),
        P("ep", None, "tp"),
        P("ep", "tp", None),
    )
    return jax.shard_map(
        on_device,
        mesh=mesh,
        in_specs=placed,
        out_specs=(P("ep", "tp"), P("ep", "tp")),
        check_vma=False,
    )
```

```python
import functools

import jax
import jax.numpy as jnp
from jax import lax
from jax.experimental import pallas as pl
from jax.experimental.pallas import tpu as pltpu
from jax.sharding import PartitionSpec as P


norm_eps = 1e-06
rope_base = 10000.0
low = -1e30
log2e = 1.4426950408889634


def vmem(count):
    return [pl.BlockSpec(memory_space=pltpu.VMEM) for _ in range(count)]


def near(x):
    return pltpu.with_memory_space_constraint(x, pltpu.VMEM)


def far(x):
    return pltpu.with_memory_space_constraint(x, pltpu.HBM)


def hbm(count):
    return [pl.BlockSpec(memory_space=pltpu.HBM) for _ in range(count)]


def start_copies(sources, targets, semaphores):
    copies = [
        pltpu.make_async_copy(a, b, semaphores.at[i])
        for i, (a, b) in enumerate(zip(sources, targets))
    ]
    for copy in copies:
        copy.start()
    return copies


def smem(count):
    return [pl.BlockSpec(memory_space=pltpu.SMEM) for _ in range(count)]


def dot_f32(a, b, dims):
    return lax.dot_general(a, b, (dims, ((), ())), preferred_element_type=jnp.float32)


chunk = 1024


def attend_kernel(ep_ref, lam_ref, *refs):
    sources, refs = refs[:4], refs[4:]
    kv_hbm = sources[3]
    out_ref, q_ref, weight_ref, gain_ref, kv_buf, top_ref, mass_ref, acc_ref = refs[:8]
    semaphores, kv_semaphores = refs[8:]
    ep = ep_ref[0]
    full = ep * 256 // chunk
    factor = (128.0**-0.5) * log2e
    copies = start_copies((sources[0],), (q_ref,), semaphores)

    def chunk_copy(j):
        at = pl.ds(pl.multiple_of(j * chunk, chunk), chunk)
        return pltpu.make_async_copy(kv_hbm.at[at, :], kv_buf.at[j], kv_semaphores.at[j])

    lax.fori_loop(0, full + 1, lambda j, c: (chunk_copy(j).start(), c)[1], 0)
    late = start_copies(
        sources[1:3], (weight_ref, gain_ref), semaphores.at[pl.ds(1, 2)]
    )
    top_ref[...] = jnp.full(top_ref.shape, low, jnp.float32)
    mass_ref[...] = jnp.zeros(mass_ref.shape, jnp.float32)
    acc_ref[...] = jnp.zeros(acc_ref.shape, jnp.float32)
    copies[0].wait()

    def fold(j, masked):
        for m in range(2):
            q = q_ref[:, 128 * m : 128 * (m + 1)]
            s = dot_f32(q, kv_buf[j, :, 128 * m : 128 * (m + 1)], ((1,), (1,)))
            if masked:
                row = ep * 256 + lax.broadcasted_iota(jnp.int32, (256, chunk), 0)
                col = j * chunk + lax.broadcasted_iota(jnp.int32, (256, chunk), 1)
                s = jnp.where(col <= row, s, low)
            pieces = [s[:, 128 * i : 128 * (i + 1)] for i in range(chunk // 128)]
            peak = jnp.max(functools.reduce(jnp.maximum, pieces), axis=1, keepdims=True)
            before = top_ref[m, :, 0:1]
            peak = jnp.maximum(peak * factor, before)
            rescale = jnp.exp2(before - peak)
            top_ref[m] = jnp.broadcast_to(peak, (256, 128))
            p = jnp.exp2(s * factor - peak)
            pieces = [p[:, 128 * i : 128 * (i + 1)] for i in range(chunk // 128)]
            mass_ref[m] = mass_ref[m] * rescale + functools.reduce(jnp.add, pieces)
            gained = dot_f32(p.astype(jnp.bfloat16), kv_buf[j, :, 256:], ((1,), (0,)))
            acc_ref[m] = acc_ref[m] * rescale + gained

    def step(j, c):
        chunk_copy(j).wait()
        fold(j, False)
        return c

    lax.fori_loop(0, full, step, 0)
    chunk_copy(full).wait()
    fold(full, True)
    maps = [acc_ref[m] / jnp.sum(mass_ref[m], axis=1, keepdims=True) for m in range(2)]
    difference = maps[0] - lam_ref[0] * maps[1]
    mean = jnp.mean(difference * difference, axis=1, keepdims=True)
    for copy in late:
        copy.wait()
    head = (difference * lax.rsqrt(mean + norm_eps) * gain_ref[...]).astype(jnp.bfloat16)
    for j in range(8):
        part = dot_f32(head, weight_ref[:, 256 * j : 256 * (j + 1)], ((1,), (0,)))
        part = part.astype(jnp.bfloat16)
        out_ref[2 * j] = part[:, :128]
        out_ref[2 * j + 1] = part[:, 128:]


def attend(ep, lam, q, kv, gain, weight):
    return pl.pallas_call(
        attend_kernel,
        out_shape=pltpu.VMEM((16, 256, 128), jnp.bfloat16),
        compiler_params=pltpu.CompilerParams(vmem_limit_bytes=40 * 2**20),
        in_specs=smem(2) + hbm(4),
        out_specs=vmem(1)[0],
        scratch_shapes=[
            pltpu.VMEM((256, 256), jnp.bfloat16),
            pltpu.VMEM(weight.shape, jnp.bfloat16),
            pltpu.VMEM((1, 256), jnp.float32),
            pltpu.VMEM((kv.shape[0] // chunk, chunk, 512), jnp.bfloat16),
            pltpu.VMEM((2, 256, 128), jnp.float32),
            pltpu.VMEM((2, 256, 128), jnp.float32),
            pltpu.VMEM((2, 256, 256), jnp.float32),
            pltpu.SemaphoreType.DMA((3,)),
            pltpu.SemaphoreType.DMA((kv.shape[0] // chunk,)),
        ],
        cost_estimate=pl.CostEstimate(
            flops=2 * 256 * kv.shape[0] * 2 * 512,
            transcendentals=256 * kv.shape[0] * 2,
            bytes_accessed=kv.shape[0] * 1024,
        ),
        name="attend",
    )(ep, lam, far(q), far(weight), far(gain.reshape(1, 256)), far(kv))


def slots_of(routes_ref):
    expert = lax.broadcasted_iota(jnp.int32, (32, 128), 0)
    first = routes_ref[0:1, :] == expert
    second = routes_ref[1:2, :] == expert
    named = jnp.where(first | second, 1.0, 0.0).astype(jnp.bfloat16)
    before = lax.broadcasted_iota(jnp.int32, (128, 128), 0)
    after = lax.broadcasted_iota(jnp.int32, (128, 128), 1)
    earlier = jnp.where(before < after, 1.0, 0.0).astype(jnp.bfloat16)
    slot = dot_f32(named, earlier, ((1,), (0,))).astype(jnp.int32)
    return first, second, slot


def chosen(named, slot):
    where = jnp.where(named, slot, -1)[:, None, :]
    index = lax.broadcasted_iota(jnp.int32, (32, 16, 128), 1)
    return jnp.where(where == index, 1.0, 0.0).reshape(512, 128).astype(jnp.bfloat16)


def begin_kernel(tp_ref, cos_ref, sin_ref, *refs):
    sources, (q_out, kv_out, packed_out), refs = refs[:6], refs[6:9], refs[9:]
    q_ref, k_ref, kv_ref, rows_ref, gain_ref, routes_ref, turned_ref = refs[:7]
    semaphores, out_semaphores = refs[7:]
    targets = (q_ref, k_ref, kv_ref.at[:, pl.ds(256, 256)], rows_ref, gain_ref, routes_ref)
    copies = start_copies(sources, targets, semaphores)
    cos_table = cos_ref[...]
    sin_table = sin_ref[...]

    def turned(x):
        x = x.astype(jnp.float32)
        return (x * cos_table + pltpu.roll(x, 64, 1) * sin_table).astype(jnp.bfloat16)

    for ref, out, copy in ((k_ref, kv_ref, copies[1]), (q_ref, turned_ref, copies[0])):
        copy.wait()
        for m in range(2):
            at = slice(128 * m, 128 * (m + 1))
            out[:, at] = turned(ref[:, at])
    copies[2].wait()
    leaving = start_copies((kv_ref, turned_ref), (kv_out, q_out), out_semaphores)

    copies[5].wait()
    first, second, slot = slots_of(routes_ref)
    pick = chosen(first | second, slot)
    copies[3].wait()
    copies[4].wait()
    x = rows_ref[...].astype(jnp.float32)
    inverse = lax.rsqrt(jnp.mean(x * x, axis=1, keepdims=True) + norm_eps)
    start = pl.multiple_of(tp_ref[0] * 128, 128)
    mine = rows_ref[:, pl.ds(start, 128)].astype(jnp.float32)
    normed = (mine * inverse * gain_ref[:, pl.ds(start, 128)]).astype(jnp.bfloat16)
    packed = dot_f32(pick, normed, ((1,), (0,)))
    packed_out[...] = packed.astype(jnp.bfloat16).reshape(32, 16, 128)
    for copy in leaving:
        copy.wait()


def begin(tp, offset, q, k, v, rows, gain, routes_t):
    count = q.shape[0]
    lane = jnp.arange(128, dtype=jnp.int32)
    inverse = rope_base ** (-2.0 * (lane % 64).astype(jnp.float32) / 128)
    positions = (offset + jnp.arange(count, dtype=jnp.int32)).astype(jnp.float32)
    angles = positions[:, None] * inverse[None, :]
    cos_table = jnp.cos(angles)
    sin_table = jnp.sin(angles) * jnp.where(lane < 64, -1.0, 1.0)[None, :]
    return pl.pallas_call(
        begin_kernel,
        out_shape=(
            pltpu.HBM((count, 256), jnp.bfloat16),
            pltpu.HBM((count, 512), jnp.bfloat16),
            pltpu.VMEM((32, 16, 128), jnp.bfloat16),
        ),
        compiler_params=pltpu.CompilerParams(vmem_limit_bytes=24 * 2**20),
        in_specs=smem(1) + vmem(2) + hbm(6),
        out_specs=(*hbm(2), *vmem(1)),
        scratch_shapes=[
            pltpu.VMEM((count, 256), jnp.bfloat16),
            pltpu.VMEM((count, 256), jnp.bfloat16),
            pltpu.VMEM((count, 512), jnp.bfloat16),
            pltpu.VMEM(rows.shape, jnp.bfloat16),
            pltpu.VMEM((1, rows.shape[1]), jnp.float32),
            pltpu.VMEM(routes_t.shape, jnp.int32),
            pltpu.VMEM((count, 256), jnp.bfloat16),
            pltpu.SemaphoreType.DMA((6,)),
            pltpu.SemaphoreType.DMA((2,)),
        ],
        name="begin",
    )(
        tp,
        near(cos_table),
        near(sin_table),
        *map(far, (q, k, v, rows, gain.reshape(1, -1), routes_t)),
    )


def dense_slots(shape, slot_dim):
    slot = lax.broadcasted_iota(jnp.int32, shape, slot_dim)
    row = lax.broadcasted_iota(jnp.int32, shape, 1 - slot_dim)
    place = jnp.where((slot & 15) < 12, (slot >> 4) * 12 + (slot & 15), -1)
    return jnp.where(place == row, 1.0, 0.0).astype(jnp.bfloat16)


def squeeze_kernel(arrived_ref, out_ref):
    slots = arrived_ref[...].reshape(512, 128)
    rows = dot_f32(dense_slots((384, 512), 1), slots, ((1,), (0,))).astype(jnp.bfloat16)
    for j in range(16):
        out_ref[j] = rows


def squeeze(arrived):
    return pl.pallas_call(
        squeeze_kernel,
        out_shape=pltpu.VMEM((16, 384, 128), jnp.bfloat16),
        compiler_params=pltpu.CompilerParams(vmem_limit_bytes=24 * 2**20),
        in_specs=vmem(1),
        out_specs=vmem(1)[0],
        name="squeeze",
    )(near(arrived))


def ffn_kernel(rows_ref, *refs):
    gate_ref, sources, (out_ref, up_ref, down_ref, semaphores) = refs[0], refs[1:3], refs[3:]
    copies = start_copies(sources, (up_ref, down_ref), semaphores)
    gate = jnp.zeros((384, 256), jnp.float32)
    up = jnp.zeros((384, 256), jnp.float32)
    for j in range(8):
        x = jnp.concatenate([rows_ref[2 * j], rows_ref[2 * j + 1]], axis=1)
        gate = gate + dot_f32(x, gate_ref[256 * j : 256 * (j + 1), :], ((1,), (0,)))
    copies[0].wait()
    for j in range(8):
        x = jnp.concatenate([rows_ref[2 * j], rows_ref[2 * j + 1]], axis=1)
        up = up + dot_f32(x, up_ref[256 * j : 256 * (j + 1), :], ((1,), (0,)))
    copies[1].wait()
    hidden = (gate / (1.0 + jnp.exp(-gate)) * up).astype(jnp.bfloat16)
    for j in range(8):
        part = dot_f32(hidden, down_ref[:, 256 * j : 256 * (j + 1)], ((1,), (0,)))
        part = part.astype(jnp.bfloat16)
        out_ref[2 * j] = part[:, :128]
        out_ref[2 * j + 1] = part[:, 128:]


def ffn(rows, gate, up, down):
    return pl.pallas_call(
        ffn_kernel,
        out_shape=pltpu.VMEM((16, 384, 128), jnp.bfloat16),
        compiler_params=pltpu.CompilerParams(vmem_limit_bytes=24 * 2**20),
        in_specs=vmem(2) + hbm(2),
        out_specs=vmem(1)[0],
        scratch_shapes=[
            pltpu.VMEM(up.shape, jnp.bfloat16),
            pltpu.VMEM(down.shape, jnp.bfloat16),
            pltpu.SemaphoreType.DMA((2,)),
        ],
        cost_estimate=pl.CostEstimate(
            flops=2 * 384 * 2048 * 768, transcendentals=384 * 256, bytes_accessed=6 * 2**20
        ),
        name="ffn",
    )(near(rows), near(gate), far(up), far(down))


def total_kernel(parts_ref, out_ref):
    total = parts_ref[0].astype(jnp.float32)
    for j in range(1, 16):
        total = total + parts_ref[j].astype(jnp.float32)
    rows = total.astype(jnp.bfloat16)
    slots = dot_f32(dense_slots((512, 384), 0), rows, ((1,), (0,)))
    out_ref[...] = slots.astype(jnp.bfloat16).reshape(32, 16, 128)


def total_of(parts):
    return pl.pallas_call(
        total_kernel,
        out_shape=pltpu.VMEM((32, 16, 128), jnp.bfloat16),
        compiler_params=pltpu.CompilerParams(vmem_limit_bytes=24 * 2**20),
        in_specs=vmem(1),
        out_specs=vmem(1)[0],
        name="total",
    )(near(parts))


def finish_kernel(parts_ref, returned_ref, routes_hbm, weights_hbm, mixed_out, expert_out, *refs):
    routes_ref, weights_ref, semaphores = refs
    copies = start_copies((routes_hbm, weights_hbm), (routes_ref, weights_ref), semaphores)
    total = parts_ref[0].astype(jnp.float32)
    for j in range(1, 16):
        total = total + parts_ref[j].astype(jnp.float32)
    mixed_out[...] = total.astype(jnp.bfloat16)
    for copy in copies:
        copy.wait()
    slots = returned_ref[...].reshape(512, 128)
    first, second, slot = slots_of(routes_ref)
    row = lax.broadcasted_iota(jnp.int32, (128, 128), 0)
    col = lax.broadcasted_iota(jnp.int32, (128, 128), 1)

    def picked(k, named):
        rows = dot_f32(chosen(named, slot), slots, ((0,), (0,)))
        weights = jnp.where(row == col, weights_ref[k : k + 1, :], 0.0)
        return jnp.sum(weights, axis=1, keepdims=True) * rows

    expert_out[...] = (picked(0, first) + picked(1, second)).astype(jnp.bfloat16)


def finish(parts, returned, routes_t, weights_t):
    return pl.pallas_call(
        finish_kernel,
        out_shape=(
            jax.ShapeDtypeStruct((256, 128), jnp.bfloat16),
            jax.ShapeDtypeStruct((128, 128), jnp.bfloat16),
        ),
        compiler_params=pltpu.CompilerParams(vmem_limit_bytes=24 * 2**20),
        in_specs=vmem(2) + hbm(2),
        out_specs=tuple(vmem(2)),
        scratch_shapes=[
            pltpu.VMEM(routes_t.shape, jnp.int32),
            pltpu.VMEM(weights_t.shape, jnp.float32),
            pltpu.SemaphoreType.DMA((2,)),
        ],
        name="finish",
    )(near(parts), near(returned), far(routes_t), far(weights_t))


def exchange(blocks, axis):
    return lax.all_to_all(blocks, axis, split_axis=0, concat_axis=0, tiled=True)


def on_device(
    query_maps,
    key_maps,
    value_rows,
    head_lambda,
    head_gain,
    out_weight,
    expert_rows,
    expert_gain,
    routes,
    route_weights,
    gate_weight,
    up_weight,
    down_weight,
):
    return step_of(
        query_maps,
        key_maps,
        value_rows,
        head_lambda,
        head_gain,
        out_weight,
        expert_rows,
        expert_gain,
        routes,
        route_weights,
        gate_weight[0],
        up_weight[0],
        down_weight[0],
    )


def step_of(
    query_maps,
    key_maps,
    value_rows,
    head_lambda,
    head_gain,
    out_weight,
    expert_rows,
    expert_gain,
    routes,
    route_weights,
    gate_weight,
    up_weight,
    down_weight,
):
    ep = lax.axis_index("ep")
    tp = lax.axis_index("tp")
    routes_t = routes.T
    own_q, own_kv, packed = begin(
        tp.reshape(1),
        ep * query_maps.shape[0],
        query_maps,
        key_maps,
        value_rows,
        expert_rows,
        expert_gain,
        routes_t,
    )
    arrived = exchange(packed, "ep")
    kv = lax.all_gather(own_kv, "ep", axis=0, tiled=True)
    gathered = exchange(squeeze(arrived), "tp")
    parts = ffn(gathered, gate_weight, up_weight, down_weight)
    summed = total_of(exchange(parts, "tp"))
    returned = exchange(summed, "ep")

    partial_value = attend(ep.reshape(1), head_lambda, own_q, kv, head_gain, out_weight)
    mixed_parts = exchange(partial_value, "tp")
    return finish(mixed_parts, returned, routes_t, route_weights.T)


def solution(mesh):
    placed = (
        P("ep", "tp"),
        P("ep", "tp"),
        P("ep", "tp"),
        P("tp"),
        P(),
        P("tp", None),
        P("ep", None),
        P(),
        P("ep", None),
        P("ep", None),
        P("ep", None, "tp"),
        P("ep", None, "tp"),
        P("ep", "tp", None),
    )
    return jax.shard_map(
        on_device,
        mesh=mesh,
        in_specs=placed,
        out_specs=(P("ep", "tp"), P("ep", "tp")),
        check_vma=False,
    )
```

```python
import functools

import jax
import jax.numpy as jnp
import numpy as np
from jax import lax
from jax.experimental import pallas as pl
from jax.experimental.pallas import tpu as pltpu
from jax.sharding import PartitionSpec as P


norm_eps = 1e-06
rope_base = 10000.0
low = -1e30
log2e = 1.4426950408889634


def vmem(count):
    return [pl.BlockSpec(memory_space=pltpu.VMEM) for _ in range(count)]


def near(x):
    return pltpu.with_memory_space_constraint(x, pltpu.VMEM)


def far(x):
    return pltpu.with_memory_space_constraint(x, pltpu.HBM)


def hbm(count):
    return [pl.BlockSpec(memory_space=pltpu.HBM) for _ in range(count)]


def start_copies(sources, targets, semaphores):
    copies = [
        pltpu.make_async_copy(a, b, semaphores.at[i])
        for i, (a, b) in enumerate(zip(sources, targets))
    ]
    for copy in copies:
        copy.start()
    return copies


def smem(count):
    return [pl.BlockSpec(memory_space=pltpu.SMEM) for _ in range(count)]


def dot_f32(a, b, dims):
    return lax.dot_general(a, b, (dims, ((), ())), preferred_element_type=jnp.float32)


chunk = 1024


def attend_kernel(ep_ref, lam_ref, *refs):
    sources, refs = refs[:4], refs[4:]
    kv_hbm = sources[3]
    out_ref, q_ref, weight_ref, gain_ref, kv_buf, top_ref, mass_ref, acc_ref = refs[:8]
    semaphores, kv_semaphores = refs[8:]
    ep = ep_ref[0]
    full = ep * 256 // chunk
    factor = (128.0**-0.5) * log2e
    copies = start_copies((sources[0],), (q_ref,), semaphores)

    def chunk_copy(j):
        at = pl.ds(pl.multiple_of(j * chunk, chunk), chunk)
        return pltpu.make_async_copy(kv_hbm.at[at, :], kv_buf.at[j], kv_semaphores.at[j])

    lax.fori_loop(0, full + 1, lambda j, c: (chunk_copy(j).start(), c)[1], 0)
    late = start_copies(
        sources[1:3], (weight_ref, gain_ref), semaphores.at[pl.ds(1, 2)]
    )
    top_ref[...] = jnp.full(top_ref.shape, low, jnp.float32)
    mass_ref[...] = jnp.zeros(mass_ref.shape, jnp.float32)
    acc_ref[...] = jnp.zeros(acc_ref.shape, jnp.float32)
    copies[0].wait()

    def fold(j, masked):
        for m in range(2):
            q = q_ref[:, 128 * m : 128 * (m + 1)]
            s = dot_f32(q, kv_buf[j, :, 128 * m : 128 * (m + 1)], ((1,), (1,)))
            if masked:
                row = ep * 256 + lax.broadcasted_iota(jnp.int32, (256, chunk), 0)
                col = j * chunk + lax.broadcasted_iota(jnp.int32, (256, chunk), 1)
                s = jnp.where(col <= row, s, low)
            pieces = [s[:, 128 * i : 128 * (i + 1)] for i in range(chunk // 128)]
            peak = jnp.max(functools.reduce(jnp.maximum, pieces), axis=1, keepdims=True)
            before = top_ref[m, :, 0:1]
            peak = jnp.maximum(peak * factor, before)
            rescale = jnp.exp2(before - peak)
            top_ref[m] = jnp.broadcast_to(peak, (256, 128))
            p = jnp.exp2(s * factor - peak)
            pieces = [p[:, 128 * i : 128 * (i + 1)] for i in range(chunk // 128)]
            mass_ref[m] = mass_ref[m] * rescale + functools.reduce(jnp.add, pieces)
            gained = dot_f32(p.astype(jnp.bfloat16), kv_buf[j, :, 256:], ((1,), (0,)))
            acc_ref[m] = acc_ref[m] * rescale + gained

    def step(j, c):
        chunk_copy(j).wait()
        fold(j, False)
        return c

    lax.fori_loop(0, full, step, 0)
    chunk_copy(full).wait()
    fold(full, True)
    maps = [acc_ref[m] / jnp.sum(mass_ref[m], axis=1, keepdims=True) for m in range(2)]
    difference = maps[0] - lam_ref[0] * maps[1]
    mean = jnp.mean(difference * difference, axis=1, keepdims=True)
    for copy in late:
        copy.wait()
    head = (difference * lax.rsqrt(mean + norm_eps) * gain_ref[...]).astype(jnp.bfloat16)
    for j in range(8):
        part = dot_f32(head, weight_ref[:, 256 * j : 256 * (j + 1)], ((1,), (0,)))
        part = part.astype(jnp.bfloat16)
        out_ref[2 * j] = part[:, :128]
        out_ref[2 * j + 1] = part[:, 128:]


def attend(ep, lam, q, kv, gain, weight):
    return pl.pallas_call(
        attend_kernel,
        out_shape=pltpu.VMEM((16, 256, 128), jnp.bfloat16),
        compiler_params=pltpu.CompilerParams(vmem_limit_bytes=40 * 2**20),
        in_specs=smem(2) + hbm(4),
        out_specs=vmem(1)[0],
        scratch_shapes=[
            pltpu.VMEM((256, 256), jnp.bfloat16),
            pltpu.VMEM(weight.shape, jnp.bfloat16),
            pltpu.VMEM((1, 256), jnp.float32),
            pltpu.VMEM((kv.shape[0] // chunk, chunk, 512), jnp.bfloat16),
            pltpu.VMEM((2, 256, 128), jnp.float32),
            pltpu.VMEM((2, 256, 128), jnp.float32),
            pltpu.VMEM((2, 256, 256), jnp.float32),
            pltpu.SemaphoreType.DMA((3,)),
            pltpu.SemaphoreType.DMA((kv.shape[0] // chunk,)),
        ],
        cost_estimate=pl.CostEstimate(
            flops=2 * 256 * kv.shape[0] * 2 * 512,
            transcendentals=256 * kv.shape[0] * 2,
            bytes_accessed=kv.shape[0] * 1024,
        ),
        name="attend",
    )(ep, lam, far(q), far(weight), far(gain.reshape(1, 256)), far(kv))


def slots_of(routes_ref):
    expert = lax.broadcasted_iota(jnp.int32, (32, 128), 0)
    first = routes_ref[0:1, :] == expert
    second = routes_ref[1:2, :] == expert
    named = jnp.where(first | second, 1.0, 0.0).astype(jnp.bfloat16)
    before = lax.broadcasted_iota(jnp.int32, (128, 128), 0)
    after = lax.broadcasted_iota(jnp.int32, (128, 128), 1)
    earlier = jnp.where(before < after, 1.0, 0.0).astype(jnp.bfloat16)
    slot = dot_f32(named, earlier, ((1,), (0,))).astype(jnp.int32)
    return first, second, slot


def chosen(named, slot):
    where = jnp.where(named, slot, -1)[:, None, :]
    index = lax.broadcasted_iota(jnp.int32, (32, 16, 128), 1)
    return jnp.where(where == index, 1.0, 0.0).reshape(512, 128).astype(jnp.bfloat16)


def begin_kernel(tp_ref, ep_ref, near_hbm, far_hbm, *refs):
    sources, (q_out, kv_out, packed_out), refs = refs[:6], refs[6:9], refs[9:]
    q_ref, k_ref, kv_ref, rows_ref, gain_ref, routes_ref, turned_ref = refs[:7]
    near_ref, far_ref, semaphores, out_semaphores, table_semaphores = refs[7:]
    tables = start_copies(
        (near_hbm, far_hbm.at[ep_ref[0]]), (near_ref, far_ref), table_semaphores
    )
    targets = (q_ref, k_ref, kv_ref.at[:, pl.ds(256, 256)], rows_ref, gain_ref, routes_ref)
    copies = start_copies(sources, targets, semaphores)
    for copy in tables:
        copy.wait()
    cos_near, sin_near = near_ref[:, :128], near_ref[:, 128:]
    cos_far, sin_far = far_ref[0:1, :], far_ref[1:2, :]
    cos_table = cos_near * cos_far - sin_near * sin_far
    sin_table = sin_near * cos_far + cos_near * sin_far
    lane = lax.broadcasted_iota(jnp.int32, sin_table.shape, 1)
    sin_table = jnp.where(lane < 64, -sin_table, sin_table)

    def turned(x):
        x = x.astype(jnp.float32)
        return (x * cos_table + pltpu.roll(x, 64, 1) * sin_table).astype(jnp.bfloat16)

    for ref, out, copy in ((k_ref, kv_ref, copies[1]), (q_ref, turned_ref, copies[0])):
        copy.wait()
        for m in range(2):
            at = slice(128 * m, 128 * (m + 1))
            out[:, at] = turned(ref[:, at])
    copies[2].wait()
    leaving = start_copies((kv_ref, turned_ref), (kv_out, q_out), out_semaphores)

    copies[5].wait()
    first, second, slot = slots_of(routes_ref)
    pick = chosen(first | second, slot)
    copies[3].wait()
    copies[4].wait()
    x = rows_ref[...].astype(jnp.float32)
    inverse = lax.rsqrt(jnp.mean(x * x, axis=1, keepdims=True) + norm_eps)
    start = pl.multiple_of(tp_ref[0] * 128, 128)
    mine = rows_ref[:, pl.ds(start, 128)].astype(jnp.float32)
    normed = (mine * inverse * gain_ref[:, pl.ds(start, 128)]).astype(jnp.bfloat16)
    packed = dot_f32(pick, normed, ((1,), (0,)))
    packed_out[...] = packed.astype(jnp.bfloat16).reshape(32, 16, 128)
    for copy in leaving:
        copy.wait()


def angle_tables(count, blocks):
    inverse = np.tile(rope_base ** (-2.0 * np.arange(64) / 128), 2)
    within = np.arange(count)[:, None] * inverse
    starts = (np.arange(blocks) * count)[:, None] * inverse
    near_table = np.concatenate([np.cos(within), np.sin(within)], axis=1)
    far_table = np.stack([np.cos(starts), np.sin(starts)], axis=1)
    return near_table.astype(np.float32), far_table.astype(np.float32)


def begin(tp, ep, blocks, q, k, v, rows, gain, routes_t):
    count = q.shape[0]
    near_table, far_table = angle_tables(count, blocks)
    return pl.pallas_call(
        begin_kernel,
        out_shape=(
            pltpu.HBM((count, 256), jnp.bfloat16),
            pltpu.HBM((count, 512), jnp.bfloat16),
            pltpu.VMEM((32, 16, 128), jnp.bfloat16),
        ),
        compiler_params=pltpu.CompilerParams(vmem_limit_bytes=24 * 2**20),
        in_specs=smem(2) + hbm(8),
        out_specs=(*hbm(2), *vmem(1)),
        scratch_shapes=[
            pltpu.VMEM((count, 256), jnp.bfloat16),
            pltpu.VMEM((count, 256), jnp.bfloat16),
            pltpu.VMEM((count, 512), jnp.bfloat16),
            pltpu.VMEM(rows.shape, jnp.bfloat16),
            pltpu.VMEM((1, rows.shape[1]), jnp.float32),
            pltpu.VMEM(routes_t.shape, jnp.int32),
            pltpu.VMEM((count, 256), jnp.bfloat16),
            pltpu.VMEM((count, 256), jnp.float32),
            pltpu.VMEM((2, 128), jnp.float32),
            pltpu.SemaphoreType.DMA((6,)),
            pltpu.SemaphoreType.DMA((2,)),
            pltpu.SemaphoreType.DMA((2,)),
        ],
        name="begin",
    )(
        tp,
        ep,
        far(jnp.asarray(near_table)),
        far(jnp.asarray(far_table)),
        *map(far, (q, k, v, rows, gain.reshape(1, -1), routes_t)),
    )


def dense_slots(shape, slot_dim):
    slot = lax.broadcasted_iota(jnp.int32, shape, slot_dim)
    row = lax.broadcasted_iota(jnp.int32, shape, 1 - slot_dim)
    place = jnp.where((slot & 15) < 12, (slot >> 4) * 12 + (slot & 15), -1)
    return jnp.where(place == row, 1.0, 0.0).astype(jnp.bfloat16)


def squeeze_kernel(arrived_ref, out_ref):
    slots = arrived_ref[...].reshape(512, 128)
    rows = dot_f32(dense_slots((384, 512), 1), slots, ((1,), (0,))).astype(jnp.bfloat16)
    for j in range(16):
        out_ref[j] = rows


def squeeze(arrived):
    return pl.pallas_call(
        squeeze_kernel,
        out_shape=pltpu.VMEM((16, 384, 128), jnp.bfloat16),
        compiler_params=pltpu.CompilerParams(vmem_limit_bytes=24 * 2**20),
        in_specs=vmem(1),
        out_specs=vmem(1)[0],
        name="squeeze",
    )(near(arrived))


def ffn_kernel(rows_ref, *refs):
    gate_ref, sources, (out_ref, up_ref, down_ref, semaphores) = refs[0], refs[1:3], refs[3:]
    copies = start_copies(sources, (up_ref, down_ref), semaphores)
    gate = jnp.zeros((384, 256), jnp.float32)
    up = jnp.zeros((384, 256), jnp.float32)
    for j in range(8):
        x = jnp.concatenate([rows_ref[2 * j], rows_ref[2 * j + 1]], axis=1)
        gate = gate + dot_f32(x, gate_ref[256 * j : 256 * (j + 1), :], ((1,), (0,)))
    copies[0].wait()
    for j in range(8):
        x = jnp.concatenate([rows_ref[2 * j], rows_ref[2 * j + 1]], axis=1)
        up = up + dot_f32(x, up_ref[256 * j : 256 * (j + 1), :], ((1,), (0,)))
    copies[1].wait()
    hidden = (gate / (1.0 + jnp.exp(-gate)) * up).astype(jnp.bfloat16)
    for j in range(8):
        part = dot_f32(hidden, down_ref[:, 256 * j : 256 * (j + 1)], ((1,), (0,)))
        part = part.astype(jnp.bfloat16)
        out_ref[2 * j] = part[:, :128]
        out_ref[2 * j + 1] = part[:, 128:]


def ffn(rows, gate, up, down):
    return pl.pallas_call(
        ffn_kernel,
        out_shape=pltpu.VMEM((16, 384, 128), jnp.bfloat16),
        compiler_params=pltpu.CompilerParams(vmem_limit_bytes=24 * 2**20),
        in_specs=vmem(2) + hbm(2),
        out_specs=vmem(1)[0],
        scratch_shapes=[
            pltpu.VMEM(up.shape, jnp.bfloat16),
            pltpu.VMEM(down.shape, jnp.bfloat16),
            pltpu.SemaphoreType.DMA((2,)),
        ],
        cost_estimate=pl.CostEstimate(
            flops=2 * 384 * 2048 * 768, transcendentals=384 * 256, bytes_accessed=6 * 2**20
        ),
        name="ffn",
    )(near(rows), near(gate), far(up), far(down))


def total_kernel(parts_ref, out_ref):
    total = parts_ref[0].astype(jnp.float32)
    for j in range(1, 16):
        total = total + parts_ref[j].astype(jnp.float32)
    rows = total.astype(jnp.bfloat16)
    slots = dot_f32(dense_slots((512, 384), 0), rows, ((1,), (0,)))
    out_ref[...] = slots.astype(jnp.bfloat16).reshape(32, 16, 128)


def total_of(parts):
    return pl.pallas_call(
        total_kernel,
        out_shape=pltpu.VMEM((32, 16, 128), jnp.bfloat16),
        compiler_params=pltpu.CompilerParams(vmem_limit_bytes=24 * 2**20),
        in_specs=vmem(1),
        out_specs=vmem(1)[0],
        name="total",
    )(near(parts))


def finish_kernel(parts_ref, returned_ref, routes_hbm, weights_hbm, mixed_out, expert_out, *refs):
    routes_ref, weights_ref, semaphores = refs
    copies = start_copies((routes_hbm, weights_hbm), (routes_ref, weights_ref), semaphores)
    total = parts_ref[0].astype(jnp.float32)
    for j in range(1, 16):
        total = total + parts_ref[j].astype(jnp.float32)
    mixed_out[...] = total.astype(jnp.bfloat16)
    for copy in copies:
        copy.wait()
    slots = returned_ref[...].reshape(512, 128)
    first, second, slot = slots_of(routes_ref)
    row = lax.broadcasted_iota(jnp.int32, (128, 128), 0)
    col = lax.broadcasted_iota(jnp.int32, (128, 128), 1)

    def picked(k, named):
        rows = dot_f32(chosen(named, slot), slots, ((0,), (0,)))
        weights = jnp.where(row == col, weights_ref[k : k + 1, :], 0.0)
        return jnp.sum(weights, axis=1, keepdims=True) * rows

    expert_out[...] = (picked(0, first) + picked(1, second)).astype(jnp.bfloat16)


def finish(parts, returned, routes_t, weights_t):
    return pl.pallas_call(
        finish_kernel,
        out_shape=(
            jax.ShapeDtypeStruct((256, 128), jnp.bfloat16),
            jax.ShapeDtypeStruct((128, 128), jnp.bfloat16),
        ),
        compiler_params=pltpu.CompilerParams(vmem_limit_bytes=24 * 2**20),
        in_specs=vmem(2) + hbm(2),
        out_specs=tuple(vmem(2)),
        scratch_shapes=[
            pltpu.VMEM(routes_t.shape, jnp.int32),
            pltpu.VMEM(weights_t.shape, jnp.float32),
            pltpu.SemaphoreType.DMA((2,)),
        ],
        name="finish",
    )(near(parts), near(returned), far(routes_t), far(weights_t))


def exchange(blocks, axis):
    return lax.all_to_all(blocks, axis, split_axis=0, concat_axis=0, tiled=True)


def on_device(
    query_maps,
    key_maps,
    value_rows,
    head_lambda,
    head_gain,
    out_weight,
    expert_rows,
    expert_gain,
    routes,
    route_weights,
    gate_weight,
    up_weight,
    down_weight,
):
    return step_of(
        query_maps,
        key_maps,
        value_rows,
        head_lambda,
        head_gain,
        out_weight,
        expert_rows,
        expert_gain,
        routes,
        route_weights,
        gate_weight[0],
        up_weight[0],
        down_weight[0],
    )


def step_of(
    query_maps,
    key_maps,
    value_rows,
    head_lambda,
    head_gain,
    out_weight,
    expert_rows,
    expert_gain,
    routes,
    route_weights,
    gate_weight,
    up_weight,
    down_weight,
):
    ep = lax.axis_index("ep")
    tp = lax.axis_index("tp")
    routes_t = routes.T
    own_q, own_kv, packed = begin(
        tp.reshape(1),
        ep.reshape(1),
        lax.axis_size("ep"),
        query_maps,
        key_maps,
        value_rows,
        expert_rows,
        expert_gain,
        routes_t,
    )
    arrived = exchange(packed, "ep")
    kv = lax.all_gather(own_kv, "ep", axis=0, tiled=True)
    gathered = exchange(squeeze(arrived), "tp")
    parts = ffn(gathered, gate_weight, up_weight, down_weight)
    summed = total_of(exchange(parts, "tp"))
    returned = exchange(summed, "ep")

    partial_value = attend(ep.reshape(1), head_lambda, own_q, kv, head_gain, out_weight)
    mixed_parts = exchange(partial_value, "tp")
    return finish(mixed_parts, returned, routes_t, route_weights.T)


def solution(mesh):
    placed = (
        P("ep", "tp"),
        P("ep", "tp"),
        P("ep", "tp"),
        P("tp"),
        P(),
        P("tp", None),
        P("ep", None),
        P(),
        P("ep", None),
        P("ep", None),
        P("ep", None, "tp"),
        P("ep", None, "tp"),
        P("ep", "tp", None),
    )
    return jax.shard_map(
        on_device,
        mesh=mesh,
        in_specs=placed,
        out_specs=(P("ep", "tp"), P("ep", "tp")),
        check_vma=False,
    )
```

```python
import functools

import jax
import jax.numpy as jnp
import numpy as np
from jax import lax
from jax.experimental import pallas as pl
from jax.experimental.pallas import tpu as pltpu
from jax.sharding import PartitionSpec as P


norm_eps = 1e-06
rope_base = 10000.0
low = -1e30
log2e = 1.4426950408889634


def vmem(count):
    return [pl.BlockSpec(memory_space=pltpu.VMEM) for _ in range(count)]


def near(x):
    return pltpu.with_memory_space_constraint(x, pltpu.VMEM)


def far(x):
    return pltpu.with_memory_space_constraint(x, pltpu.HBM)


def hbm(count):
    return [pl.BlockSpec(memory_space=pltpu.HBM) for _ in range(count)]


def start_copies(sources, targets, semaphores):
    copies = [
        pltpu.make_async_copy(a, b, semaphores.at[i])
        for i, (a, b) in enumerate(zip(sources, targets))
    ]
    for copy in copies:
        copy.start()
    return copies


def smem(count):
    return [pl.BlockSpec(memory_space=pltpu.SMEM) for _ in range(count)]


def dot_f32(a, b, dims):
    return lax.dot_general(a, b, (dims, ((), ())), preferred_element_type=jnp.float32)


chunk = 1024


def attend_kernel(ep_ref, lam_ref, *refs):
    sources, refs = refs[:4], refs[4:]
    kv_hbm = sources[3]
    out_ref, q_ref, weight_ref, gain_ref, kv_buf, top_ref, mass_ref, acc_ref = refs[:8]
    semaphores, kv_semaphores = refs[8:]
    ep = ep_ref[0]
    full = ep * 256 // chunk
    factor = (128.0**-0.5) * log2e
    copies = start_copies((sources[0],), (q_ref,), semaphores)

    def chunk_copy(j):
        at = pl.ds(pl.multiple_of(j * chunk, chunk), chunk)
        return pltpu.make_async_copy(kv_hbm.at[at, :], kv_buf.at[j], kv_semaphores.at[j])

    lax.fori_loop(0, full + 1, lambda j, c: (chunk_copy(j).start(), c)[1], 0)
    late = start_copies(
        sources[1:3], (weight_ref, gain_ref), semaphores.at[pl.ds(1, 2)]
    )
    top_ref[...] = jnp.full(top_ref.shape, low, jnp.float32)
    mass_ref[...] = jnp.zeros(mass_ref.shape, jnp.float32)
    acc_ref[...] = jnp.zeros(acc_ref.shape, jnp.float32)
    copies[0].wait()

    def fold(j, masked):
        for m in range(2):
            q = q_ref[:, 128 * m : 128 * (m + 1)]
            s = dot_f32(q, kv_buf[j, :, 128 * m : 128 * (m + 1)], ((1,), (1,)))
            if masked:
                row = ep * 256 + lax.broadcasted_iota(jnp.int32, (256, chunk), 0)
                col = j * chunk + lax.broadcasted_iota(jnp.int32, (256, chunk), 1)
                s = jnp.where(col <= row, s, low)
            pieces = [s[:, 128 * i : 128 * (i + 1)] for i in range(chunk // 128)]
            peak = jnp.max(functools.reduce(jnp.maximum, pieces), axis=1, keepdims=True)
            before = top_ref[m, :, 0:1]
            peak = jnp.maximum(peak * factor, before)
            rescale = jnp.exp2(before - peak)
            top_ref[m] = jnp.broadcast_to(peak, (256, 128))
            p = jnp.exp2(s * factor - peak)
            pieces = [p[:, 128 * i : 128 * (i + 1)] for i in range(chunk // 128)]
            mass_ref[m] = mass_ref[m] * rescale + functools.reduce(jnp.add, pieces)
            gained = dot_f32(p.astype(jnp.bfloat16), kv_buf[j, :, 256:], ((1,), (0,)))
            acc_ref[m] = acc_ref[m] * rescale + gained

    def step(j, c):
        chunk_copy(j).wait()
        fold(j, False)
        return c

    lax.fori_loop(0, full, step, 0)
    chunk_copy(full).wait()
    fold(full, True)
    maps = [acc_ref[m] / jnp.sum(mass_ref[m], axis=1, keepdims=True) for m in range(2)]
    difference = maps[0] - lam_ref[0] * maps[1]
    mean = jnp.mean(difference * difference, axis=1, keepdims=True)
    for copy in late:
        copy.wait()
    head = (difference * lax.rsqrt(mean + norm_eps) * gain_ref[...]).astype(jnp.bfloat16)
    for j in range(8):
        part = dot_f32(head, weight_ref[:, 256 * j : 256 * (j + 1)], ((1,), (0,)))
        part = part.astype(jnp.bfloat16)
        out_ref[2 * j] = part[:, :128]
        out_ref[2 * j + 1] = part[:, 128:]


def attend(ep, lam, q, kv, gain, weight):
    return pl.pallas_call(
        attend_kernel,
        out_shape=pltpu.VMEM((16, 256, 128), jnp.bfloat16),
        compiler_params=pltpu.CompilerParams(vmem_limit_bytes=40 * 2**20),
        in_specs=smem(2) + hbm(4),
        out_specs=vmem(1)[0],
        scratch_shapes=[
            pltpu.VMEM((256, 256), jnp.bfloat16),
            pltpu.VMEM(weight.shape, jnp.bfloat16),
            pltpu.VMEM((1, 256), jnp.float32),
            pltpu.VMEM((kv.shape[0] // chunk, chunk, 512), jnp.bfloat16),
            pltpu.VMEM((2, 256, 128), jnp.float32),
            pltpu.VMEM((2, 256, 128), jnp.float32),
            pltpu.VMEM((2, 256, 256), jnp.float32),
            pltpu.SemaphoreType.DMA((3,)),
            pltpu.SemaphoreType.DMA((kv.shape[0] // chunk,)),
        ],
        cost_estimate=pl.CostEstimate(
            flops=2 * 256 * kv.shape[0] * 2 * 512,
            transcendentals=256 * kv.shape[0] * 2,
            bytes_accessed=kv.shape[0] * 1024,
        ),
        name="attend",
    )(ep, lam, far(q), far(weight), far(gain.reshape(1, 256)), far(kv))


def slots_of(routes_ref):
    expert = lax.broadcasted_iota(jnp.int32, (32, 128), 0)
    first = routes_ref[0:1, :] == expert
    second = routes_ref[1:2, :] == expert
    named = jnp.where(first | second, 1.0, 0.0).astype(jnp.bfloat16)
    before = lax.broadcasted_iota(jnp.int32, (128, 128), 0)
    after = lax.broadcasted_iota(jnp.int32, (128, 128), 1)
    earlier = jnp.where(before < after, 1.0, 0.0).astype(jnp.bfloat16)
    slot = dot_f32(named, earlier, ((1,), (0,))).astype(jnp.int32)
    return first, second, slot


def chosen(named, slot):
    where = jnp.where(named, slot, -1)[:, None, :]
    index = lax.broadcasted_iota(jnp.int32, (32, 16, 128), 1)
    return jnp.where(where == index, 1.0, 0.0).reshape(512, 128).astype(jnp.bfloat16)


def begin_kernel(tp_ref, ep_ref, near_hbm, far_hbm, *refs):
    sources, (q_out, kv_out, packed_out), refs = refs[:6], refs[6:9], refs[9:]
    q_ref, k_ref, kv_ref, rows_ref, gain_ref, routes_ref, turned_ref = refs[:7]
    near_ref, far_ref, semaphores, out_semaphores, table_semaphores = refs[7:]
    tables = start_copies(
        (near_hbm, far_hbm.at[ep_ref[0]]), (near_ref, far_ref), table_semaphores
    )
    targets = (q_ref, k_ref, kv_ref.at[:, pl.ds(256, 256)], rows_ref, gain_ref, routes_ref)
    copies = start_copies(sources, targets, semaphores)
    for copy in tables:
        copy.wait()
    cos_near, sin_near = near_ref[:, :128], near_ref[:, 128:]
    cos_far, sin_far = far_ref[0:1, :], far_ref[1:2, :]
    cos_table = cos_near * cos_far - sin_near * sin_far
    sin_table = sin_near * cos_far + cos_near * sin_far
    lane = lax.broadcasted_iota(jnp.int32, sin_table.shape, 1)
    sin_table = jnp.where(lane < 64, -sin_table, sin_table)

    def turned(x):
        x = x.astype(jnp.float32)
        return (x * cos_table + pltpu.roll(x, 64, 1) * sin_table).astype(jnp.bfloat16)

    for ref, out, copy in ((k_ref, kv_ref, copies[1]), (q_ref, turned_ref, copies[0])):
        copy.wait()
        for m in range(2):
            at = slice(128 * m, 128 * (m + 1))
            out[:, at] = turned(ref[:, at])
    copies[2].wait()
    leaving = start_copies((kv_ref, turned_ref), (kv_out, q_out), out_semaphores)

    copies[5].wait()
    first, second, slot = slots_of(routes_ref)
    pick = chosen(first | second, slot)
    copies[3].wait()
    copies[4].wait()
    x = rows_ref[...].astype(jnp.float32)
    inverse = lax.rsqrt(jnp.mean(x * x, axis=1, keepdims=True) + norm_eps)
    start = pl.multiple_of(tp_ref[0] * 128, 128)
    mine = rows_ref[:, pl.ds(start, 128)].astype(jnp.float32)
    normed = (mine * inverse * gain_ref[:, pl.ds(start, 128)]).astype(jnp.bfloat16)
    packed = dot_f32(pick, normed, ((1,), (0,)))
    packed_out[...] = packed.astype(jnp.bfloat16).reshape(32, 16, 128)
    for copy in leaving:
        copy.wait()


def angle_tables(count, blocks):
    inverse = np.tile(rope_base ** (-2.0 * np.arange(64) / 128), 2)
    within = np.arange(count)[:, None] * inverse
    starts = (np.arange(blocks) * count)[:, None] * inverse
    near_table = np.concatenate([np.cos(within), np.sin(within)], axis=1)
    far_table = np.stack([np.cos(starts), np.sin(starts)], axis=1)
    return near_table.astype(np.float32), far_table.astype(np.float32)


def begin(tp, ep, blocks, q, k, v, rows, gain, routes_t):
    count = q.shape[0]
    near_table, far_table = angle_tables(count, blocks)
    return pl.pallas_call(
        begin_kernel,
        out_shape=(
            pltpu.HBM((count, 256), jnp.bfloat16),
            pltpu.HBM((count, 512), jnp.bfloat16),
            pltpu.VMEM((32, 16, 128), jnp.bfloat16),
        ),
        compiler_params=pltpu.CompilerParams(vmem_limit_bytes=24 * 2**20),
        in_specs=smem(2) + hbm(8),
        out_specs=(*hbm(2), *vmem(1)),
        scratch_shapes=[
            pltpu.VMEM((count, 256), jnp.bfloat16),
            pltpu.VMEM((count, 256), jnp.bfloat16),
            pltpu.VMEM((count, 512), jnp.bfloat16),
            pltpu.VMEM(rows.shape, jnp.bfloat16),
            pltpu.VMEM((1, rows.shape[1]), jnp.float32),
            pltpu.VMEM(routes_t.shape, jnp.int32),
            pltpu.VMEM((count, 256), jnp.bfloat16),
            pltpu.VMEM((count, 256), jnp.float32),
            pltpu.VMEM((2, 128), jnp.float32),
            pltpu.SemaphoreType.DMA((6,)),
            pltpu.SemaphoreType.DMA((2,)),
            pltpu.SemaphoreType.DMA((2,)),
        ],
        name="begin",
    )(
        tp,
        ep,
        far(jnp.asarray(near_table)),
        far(jnp.asarray(far_table)),
        *map(far, (q, k, v, rows, gain.reshape(1, -1), routes_t)),
    )


def dense_slots(shape, slot_dim):
    slot = lax.broadcasted_iota(jnp.int32, shape, slot_dim)
    row = lax.broadcasted_iota(jnp.int32, shape, 1 - slot_dim)
    place = jnp.where((slot & 15) < 12, (slot >> 4) * 12 + (slot & 15), -1)
    return jnp.where(place == row, 1.0, 0.0).astype(jnp.bfloat16)


def squeeze_kernel(arrived_ref, out_ref):
    slots = arrived_ref[...].reshape(512, 128)
    rows = dot_f32(dense_slots((384, 512), 1), slots, ((1,), (0,))).astype(jnp.bfloat16)
    for j in range(16):
        out_ref[j] = rows


def squeeze(arrived):
    return pl.pallas_call(
        squeeze_kernel,
        out_shape=pltpu.VMEM((16, 384, 128), jnp.bfloat16),
        compiler_params=pltpu.CompilerParams(vmem_limit_bytes=24 * 2**20),
        in_specs=vmem(1),
        out_specs=vmem(1)[0],
        name="squeeze",
    )(near(arrived))


def ffn_kernel(rows_ref, *refs):
    gate_ref, sources, (out_ref, up_ref, down_ref, semaphores) = refs[0], refs[1:3], refs[3:]
    copies = start_copies(sources, (up_ref, down_ref), semaphores)
    gate = jnp.zeros((384, 256), jnp.float32)
    up = jnp.zeros((384, 256), jnp.float32)
    for j in range(8):
        x = jnp.concatenate([rows_ref[2 * j], rows_ref[2 * j + 1]], axis=1)
        gate = gate + dot_f32(x, gate_ref[256 * j : 256 * (j + 1), :], ((1,), (0,)))
    copies[0].wait()
    for j in range(8):
        x = jnp.concatenate([rows_ref[2 * j], rows_ref[2 * j + 1]], axis=1)
        up = up + dot_f32(x, up_ref[256 * j : 256 * (j + 1), :], ((1,), (0,)))
    copies[1].wait()
    hidden = (gate / (1.0 + jnp.exp(-gate)) * up).astype(jnp.bfloat16)
    for j in range(8):
        part = dot_f32(hidden, down_ref[:, 256 * j : 256 * (j + 1)], ((1,), (0,)))
        part = part.astype(jnp.bfloat16)
        out_ref[2 * j] = part[:, :128]
        out_ref[2 * j + 1] = part[:, 128:]


def ffn(rows, gate, up, down):
    return pl.pallas_call(
        ffn_kernel,
        out_shape=pltpu.VMEM((16, 384, 128), jnp.bfloat16),
        compiler_params=pltpu.CompilerParams(vmem_limit_bytes=24 * 2**20),
        in_specs=vmem(2) + hbm(2),
        out_specs=vmem(1)[0],
        scratch_shapes=[
            pltpu.VMEM(up.shape, jnp.bfloat16),
            pltpu.VMEM(down.shape, jnp.bfloat16),
            pltpu.SemaphoreType.DMA((2,)),
        ],
        cost_estimate=pl.CostEstimate(
            flops=2 * 384 * 2048 * 768, transcendentals=384 * 256, bytes_accessed=6 * 2**20
        ),
        name="ffn",
    )(near(rows), near(gate), far(up), far(down))


def total_kernel(parts_ref, out_ref):
    total = parts_ref[0].astype(jnp.float32)
    for j in range(1, 16):
        total = total + parts_ref[j].astype(jnp.float32)
    rows = total.astype(jnp.bfloat16)
    slots = dot_f32(dense_slots((512, 384), 0), rows, ((1,), (0,)))
    out_ref[...] = slots.astype(jnp.bfloat16).reshape(32, 16, 128)


def total_of(parts):
    return pl.pallas_call(
        total_kernel,
        out_shape=pltpu.VMEM((32, 16, 128), jnp.bfloat16),
        compiler_params=pltpu.CompilerParams(vmem_limit_bytes=24 * 2**20),
        in_specs=vmem(1),
        out_specs=vmem(1)[0],
        name="total",
    )(near(parts))


def plan_kernel(routes_ref, weights_ref, one_out, two_out, scale_out):
    first, second, slot = slots_of(routes_ref)
    index = lax.broadcasted_iota(jnp.int32, (32, 16, 128), 1)
    for named, out in ((first, one_out), (second, two_out)):
        where = jnp.where(named, slot, -1)[:, None, :]
        pick = jnp.where(where == index, 1.0, 0.0).reshape(512, 128)
        out[...] = pick.T.astype(jnp.bfloat16)
    row = lax.broadcasted_iota(jnp.int32, (128, 128), 0)
    col = lax.broadcasted_iota(jnp.int32, (128, 128), 1)
    for k in range(2):
        weights = jnp.where(row == col, weights_ref[k : k + 1, :], 0.0)
        column = jnp.sum(weights, axis=1, keepdims=True)
        scale_out[:, 128 * k : 128 * (k + 1)] = jnp.broadcast_to(column, (128, 128))


def plan(routes_t, weights_t):
    return pl.pallas_call(
        plan_kernel,
        out_shape=(
            pltpu.VMEM((128, 512), jnp.bfloat16),
            pltpu.VMEM((128, 512), jnp.bfloat16),
            pltpu.VMEM((128, 256), jnp.float32),
        ),
        compiler_params=pltpu.CompilerParams(vmem_limit_bytes=24 * 2**20),
        in_specs=vmem(2),
        out_specs=tuple(vmem(3)),
        name="plan",
    )(far(routes_t), far(weights_t))


def finish_kernel(parts_ref, returned_ref, one_ref, two_ref, scale_ref, mixed_out, expert_out):
    total = parts_ref[0].astype(jnp.float32)
    for j in range(1, 16):
        total = total + parts_ref[j].astype(jnp.float32)
    mixed_out[...] = total.astype(jnp.bfloat16)
    slots = returned_ref[...].reshape(512, 128)
    one = dot_f32(one_ref[...], slots, ((1,), (0,)))
    two = dot_f32(two_ref[...], slots, ((1,), (0,)))
    expert_out[...] = (scale_ref[:, :128] * one + scale_ref[:, 128:] * two).astype(jnp.bfloat16)


def finish(parts, returned, planned):
    return pl.pallas_call(
        finish_kernel,
        out_shape=(
            jax.ShapeDtypeStruct((256, 128), jnp.bfloat16),
            jax.ShapeDtypeStruct((128, 128), jnp.bfloat16),
        ),
        compiler_params=pltpu.CompilerParams(vmem_limit_bytes=24 * 2**20),
        in_specs=vmem(5),
        out_specs=tuple(vmem(2)),
        name="finish",
    )(near(parts), near(returned), *map(near, planned))


def exchange(blocks, axis):
    return lax.all_to_all(blocks, axis, split_axis=0, concat_axis=0, tiled=True)


def on_device(
    query_maps,
    key_maps,
    value_rows,
    head_lambda,
    head_gain,
    out_weight,
    expert_rows,
    expert_gain,
    routes,
    route_weights,
    gate_weight,
    up_weight,
    down_weight,
):
    return step_of(
        query_maps,
        key_maps,
        value_rows,
        head_lambda,
        head_gain,
        out_weight,
        expert_rows,
        expert_gain,
        routes,
        route_weights,
        gate_weight[0],
        up_weight[0],
        down_weight[0],
    )


def step_of(
    query_maps,
    key_maps,
    value_rows,
    head_lambda,
    head_gain,
    out_weight,
    expert_rows,
    expert_gain,
    routes,
    route_weights,
    gate_weight,
    up_weight,
    down_weight,
):
    ep = lax.axis_index("ep")
    tp = lax.axis_index("tp")
    routes_t = routes.T
    own_q, own_kv, packed = begin(
        tp.reshape(1),
        ep.reshape(1),
        lax.axis_size("ep"),
        query_maps,
        key_maps,
        value_rows,
        expert_rows,
        expert_gain,
        routes_t,
    )
    arrived = exchange(packed, "ep")
    kv = lax.all_gather(own_kv, "ep", axis=0, tiled=True)
    gathered = exchange(squeeze(arrived), "tp")
    parts = ffn(gathered, gate_weight, up_weight, down_weight)
    summed = total_of(exchange(parts, "tp"))
    returned = exchange(summed, "ep")

    partial_value = attend(ep.reshape(1), head_lambda, own_q, kv, head_gain, out_weight)
    mixed_parts = exchange(partial_value, "tp")
    return finish(mixed_parts, returned, plan(routes_t, route_weights.T))


def solution(mesh):
    placed = (
        P("ep", "tp"),
        P("ep", "tp"),
        P("ep", "tp"),
        P("tp"),
        P(),
        P("tp", None),
        P("ep", None),
        P(),
        P("ep", None),
        P("ep", None),
        P("ep", None, "tp"),
        P("ep", None, "tp"),
        P("ep", "tp", None),
    )
    return jax.shard_map(
        on_device,
        mesh=mesh,
        in_specs=placed,
        out_specs=(P("ep", "tp"), P("ep", "tp")),
        check_vma=False,
    )
```
